32 devices in a mesh: sp: 16 (over z, y, core), tp: 2 (over x).
Axes of the slice: x: 2, y: 2, z: 4, core: 2. Of those that a mesh axis runs over, the one named last changes fastest.
Arguments:
- tokens: bfloat16 [4096, 2048], P('sp', 'tp'), may hold values from -64 to 64
- input_norm_gain: float32 [2048], replicated, may hold values from 0.1 to 1.9
- attention_query_weight: bfloat16 [2048, 512], P(None, 'tp'), may hold values from -0.21875 to 0.21875
- attention_key_weight: bfloat16 [2048, 512], P(None, 'tp'), may hold values from -0.21875 to 0.21875
- attention_value_weight: bfloat16 [2048, 512], P(None, 'tp'), may hold values from -0.125 to 0.125
- attention_score_bias: float32 [8], P('tp'), may hold values from -18 to -7
- recurrence_query_weight: bfloat16 [2048, 1024], P(None, 'tp'), may hold values from -0.125 to 0.125
- forget_weight: bfloat16 [2048, 1024], P(None, 'tp'), may hold values from -0.125 to 0.125
- input_weight: bfloat16 [2048, 512], P(None, 'tp'), may hold values from -0.125 to 0.125
- output_gate_weight: bfloat16 [2048, 512], P(None, 'tp'), may hold values from -0.125 to 0.125
- forget_minimum: float32 [8, 128], P('tp'), may hold values from 0.9 to 1
- decay_spikes: float32 [4096, 8], P('sp', 'tp'), may hold values from -2.2 to 0
- head_norm_gain: float32 [64], replicated, may hold values from 0.1 to 1.9
- attention_output_weight: bfloat16 [512, 2048], P('tp'), may hold values from -0.25 to 0.25
- recurrence_output_weight: bfloat16 [512, 2048], P('tp'), may hold values from -0.25 to 0.25
Outputs:
- mixed: bfloat16 [4096, 2048], P('sp', 'tp')
The draws below stay inside these ranges and needn't reach their ends.
All inputs are finite; a program needn't handle non-finite values.
Results may differ from the reference program's by a relative error of at most 0.018.
Values may be sent and summed in bfloat16 or wider, within the bound.
A program may use at most 64 MiB of HBM per device.

```python
import jax
import jax.numpy as jnp
from jax import lax

D = 2048
SB_HEADS = 8
HEAD = 64
REC_HEADS = 8
REC_KEY = 128
REC_VAL = 64
TOK_DEV = 256
REC_SPAN = 64
TOKENS = 4096


def draw_tokens(key, part):
    streams = jax.random.split(jax.random.fold_in(key, 11), 3)
    column_rise = jnp.exp(jnp.log(4.0) * jnp.arange(D, dtype=jnp.float32) / D)
    column_rough = jnp.exp(jax.random.uniform(streams[0], (D,), jnp.float32, -0.35, 0.35))
    row_scale = jnp.exp(jax.random.uniform(streams[1], (TOKENS, 1), jnp.float32, -0.7, 0.7))
    noise_field = jnp.clip(jax.random.normal(streams[2], (TOKENS, D), jnp.float32), -5.0, 5.0)
    return (noise_field * row_scale * column_rise[None, :] * column_rough[None, :]).astype(jnp.bfloat16)


def draw_attention_score_bias(key, part):
    spread = jax.random.uniform(jax.random.fold_in(key, 23), (SB_HEADS,), jnp.float32, jnp.log(0.3), jnp.log(3.0))
    return spread - jnp.log(90.0 * TOKENS)


def draw_forget_minimum(key, part):
    streams = jax.random.split(jax.random.fold_in(key, 31), 3)
    ranking = jax.random.permutation(streams[0], REC_HEADS)
    slow_count = REC_HEADS // 2
    is_slow = (ranking < slow_count)[:, None]
    slow_gap = jnp.exp(jax.random.uniform(streams[1], (REC_HEADS, REC_KEY), jnp.float32, jnp.log(0.2), jnp.log(1.2))) / TOKENS
    fast_gap = jnp.exp(jax.random.uniform(streams[2], (REC_HEADS, REC_KEY), jnp.float32, jnp.log(0.04), jnp.log(0.1)))
    return 1.0 - jnp.where(is_slow, slow_gap, fast_gap)


def draw_decay_spikes(key, part):
    streams = jax.random.split(jax.random.fold_in(key, 47), 3)
    block_count = TOKENS // TOK_DEV
    block_rate = jnp.exp(jax.random.uniform(streams[0], (block_count, 1, REC_HEADS), jnp.float32, jnp.log(0.15), jnp.log(0.6))) / TOKENS
    steady = -jnp.broadcast_to(block_rate, (block_count, TOK_DEV, REC_HEADS)).reshape(TOKENS, REC_HEADS)
    places = jax.random.randint(streams[1], (3, REC_HEADS), 0, TOKENS)
    struck = jnp.arange(TOKENS, dtype=jnp.int32)[:, None, None] == places[None]
    depth = jnp.log(jax.random.uniform(streams[2], (3, REC_HEADS), jnp.float32, 0.5, 0.8))
    return steady + jnp.sum(jnp.where(struck, depth[None], 0.0), axis=1)


def steps_of(rng, shape, cuts, low, top_value):
    def one(dim, blocks):
        heights = jax.random.uniform(jax.random.fold_in(jax.random.fold_in(rng, 6), dim), (blocks,), jnp.float32, low / len(cuts), top_value / len(cuts))
        return jnp.repeat(jnp.exp(heights), shape[dim] // blocks).reshape((-1,) + (1,) * (len(shape) - dim - 1))

    gain = one(*cuts[0])
    for cut in cuts[1:]:
        gain = gain * one(*cut)
    return gain


def normal_values(rng, extent, scale, reach, cuts=(), kind=jnp.bfloat16):
    entries = jax.random.normal(rng, extent, jnp.float32) * scale
    if len(cuts) > 0:
        entries = steps_of(rng, extent, cuts, -0.22, 0.18) * entries
    return jnp.clip(entries, min=-reach, max=reach).astype(kind)


def setup_inputs(seed: int = 0) -> dict:
    arg_keys = jax.random.split(jax.random.key(seed), 16)
    return {
        "tokens": draw_tokens(jax.random.fold_in(arg_keys[15], 71), 0),
        "input_norm_gain": jnp.clip(1.0 + 0.18 * jax.random.normal(arg_keys[1], (D,), jnp.float32), 0.1, 1.9),
        "attention_query_weight": normal_values(arg_keys[2], (D, SB_HEADS * HEAD), (D // 3) ** -0.5, 0.21875, ((1, 2),)),
        "attention_key_weight": normal_values(arg_keys[3], (D, SB_HEADS * HEAD), (D // 3) ** -0.5, 0.21875, ((1, 2),)),
        "attention_value_weight": normal_values(arg_keys[4], (D, SB_HEADS * HEAD), D ** -0.5, 0.125, ((1, 2),)),
        "attention_score_bias": draw_attention_score_bias(jax.random.fold_in(arg_keys[15], 71), 0),
        "recurrence_query_weight": normal_values(arg_keys[6], (D, REC_HEADS * REC_KEY), D ** -0.5, 0.125, ((1, 2),)),
        "forget_weight": normal_values(arg_keys[7], (D, REC_HEADS * REC_KEY), D ** -0.5, 0.125, ((1, 2),)),
        "input_weight": normal_values(arg_keys[8], (D, REC_HEADS * REC_VAL), D ** -0.5, 0.125, ((1, 2),)),
        "output_gate_weight": normal_values(arg_keys[9], (D, REC_HEADS * REC_VAL), D ** -0.5, 0.125, ((1, 2),)),
        "forget_minimum": draw_forget_minimum(jax.random.fold_in(arg_keys[15], 71), 0),
        "decay_spikes": draw_decay_spikes(jax.random.fold_in(arg_keys[15], 71), 0),
        "head_norm_gain": jnp.clip(1.0 + 0.18 * jax.random.normal(arg_keys[12], (REC_VAL,), jnp.float32), 0.1, 1.9),
        "attention_output_weight": normal_values(arg_keys[13], (SB_HEADS * HEAD, D), (SB_HEADS * HEAD) ** -0.5, 0.25, ((0, 2),)),
        "recurrence_output_weight": normal_values(arg_keys[14], (REC_HEADS * REC_VAL, D), (REC_HEADS * REC_VAL) ** -0.5, 0.25, ((0, 2),)),
    }


epsilon = 1e-06

def project(scaled, inverse, weight):
    return (jnp.dot(scaled, weight, preferred_element_type=jnp.float32) * inverse).astype(jnp.bfloat16)

def stick_breaking(query_stick, key_stick, value_stick, attention_score_bias):
    block_count = TOKENS // TOK_DEV
    query_blocks = query_stick.reshape(block_count, TOK_DEV, SB_HEADS, HEAD)
    key_heads = key_stick.reshape(TOKENS, SB_HEADS, HEAD).astype(jnp.float32)
    value_heads = value_stick.reshape(TOKENS, SB_HEADS, HEAD).astype(jnp.float32)
    key_pos = jnp.arange(TOKENS, dtype=jnp.int32)

    def one_block(inputs):
        query_block, number = inputs
        query_pos = number * TOK_DEV + jnp.arange(TOK_DEV, dtype=jnp.int32)
        scores = jnp.einsum('qhd,khd->hqk', query_block.astype(jnp.float32), key_heads) * HEAD ** (-0.5)
        scores = scores + attention_score_bias[:, None, None]
        before = (key_pos[None, :] < query_pos[:, None])[None]
        log_rest = jnp.where(before, jax.nn.log_sigmoid(-scores), 0.0)
        later_sum = lax.cumsum(log_rest, axis=2, reverse=True) - log_rest
        weights = jnp.where(before, jnp.exp(jax.nn.log_sigmoid(scores) + later_sum), 0.0).astype(jnp.bfloat16)
        final_output = jnp.einsum('hqk,khd->qhd', weights.astype(jnp.float32), value_heads)
        return final_output.reshape(TOK_DEV, SB_HEADS * HEAD).astype(jnp.bfloat16)
    blocks = lax.map(one_block, (query_blocks, jnp.arange(block_count, dtype=jnp.int32)))
    return blocks.reshape(TOKENS, SB_HEADS * HEAD)

def linear_recurrence(query_rows, forget_rows, input_rows, gate_rows, forget_minimum, decay_spikes, head_norm_gain):
    peak_value = lax.Precision.HIGHEST
    raised_values = jax.nn.silu(query_rows.astype(jnp.float32)).reshape(TOKENS, REC_HEADS, REC_KEY)
    admitted_input = (1.0 - forget_minimum)[None] * jax.nn.sigmoid(-forget_rows.astype(jnp.float32).reshape(TOKENS, REC_HEADS, REC_KEY))
    forget_logarithm = jnp.log1p(-admitted_input) + decay_spikes[:, :, None]
    inputs = input_rows.astype(jnp.float32).reshape(TOKENS, REC_HEADS, REC_VAL)
    span_count = TOKENS // REC_SPAN
    causal = jnp.tril(jnp.ones((REC_SPAN, REC_SPAN), jnp.bool_))[:, :, None, None]

    def to_spans(array):
        return array.reshape(span_count, REC_SPAN, REC_HEADS, array.shape[-1])

    def advance(recurrent_memory, pieces):
        window_query, window_admitted, window_input, span_log = pieces
        running_total = jnp.cumsum(span_log, axis=0)
        log_gaps = running_total[:, None] - running_total[None, :]
        decay_table = jnp.where(causal, jnp.exp(jnp.where(causal, log_gaps, 0.0)), 0.0)
        inner_scores = jnp.einsum('thk,shk,tshk->hts', window_query, window_admitted, decay_table, precision=peak_value)
        final_output = jnp.einsum('hts,shv->thv', inner_scores, window_input, precision=peak_value)
        final_output = final_output + jnp.einsum('zbg,bgp->zbp', window_query * jnp.exp(running_total), recurrent_memory, precision=peak_value)
        window_total = running_total[-1]
        recurrent_memory = recurrent_memory * jnp.exp(window_total)[:, :, None] + jnp.einsum('rof,roi->ofi', window_admitted * jnp.exp(window_total[None] - running_total), window_input, precision=peak_value)
        return (recurrent_memory, final_output)
    start_memory = jnp.zeros((REC_HEADS, REC_KEY, REC_VAL), jnp.float32)
    memory_end, outputs = lax.scan(advance, start_memory, (to_spans(raised_values), to_spans(admitted_input), to_spans(inputs), to_spans(forget_logarithm)))
    outputs = outputs.reshape(TOKENS, REC_HEADS, REC_VAL)
    normed = outputs * lax.rsqrt(lax.optimization_barrier(jnp.mean(outputs * outputs, axis=2, keepdims=True)) + epsilon) * head_norm_gain
    gated_out = normed * jax.nn.silu(gate_rows.astype(jnp.float32).reshape(TOKENS, REC_HEADS, REC_VAL))
    return gated_out.reshape(TOKENS, REC_HEADS * REC_VAL).astype(jnp.bfloat16)

def reference(tokens, input_norm_gain, attention_query_weight, attention_key_weight, attention_value_weight, attention_score_bias, recurrence_query_weight, forget_weight, input_weight, output_gate_weight, forget_minimum, decay_spikes, head_norm_gain, attention_output_weight, recurrence_output_weight):
    values = tokens.astype(jnp.float32)
    scaled = (values * input_norm_gain[None, :]).astype(jnp.bfloat16)
    inverse = lax.rsqrt(lax.optimization_barrier(jnp.mean(values * values, axis=1, keepdims=True)) + epsilon)
    query_stick = project(scaled, inverse, attention_query_weight)
    key_stick = project(scaled, inverse, attention_key_weight)
    value_stick = project(scaled, inverse, attention_value_weight)
    query_rows = project(scaled, inverse, recurrence_query_weight)
    forget_rows = project(scaled, inverse, forget_weight)
    input_rows = project(scaled, inverse, input_weight)
    gate_rows = project(scaled, inverse, output_gate_weight)
    stick_heads = stick_breaking(query_stick, key_stick, value_stick, attention_score_bias)
    recurrence_heads = linear_recurrence(query_rows, forget_rows, input_rows, gate_rows, forget_minimum, decay_spikes, head_norm_gain)
    mixed_out = jnp.dot(stick_heads, attention_output_weight, preferred_element_type=jnp.float32)
    mixed_out = mixed_out + jnp.dot(recurrence_heads, recurrence_output_weight, preferred_element_type=jnp.float32)
    return mixed_out.astype(jnp.bfloat16)
```

```python
import functools
import math
import types

import jax
import jax.numpy as jnp
from jax import lax
from jax.experimental import pallas as pl
from jax.experimental.pallas import tpu as pltpu
from jax.sharding import PartitionSpec as P

HEAD = 64
REC_KEY = 128
REC_VAL = 64
LANES = 128
GROUP = 4
TAIL = 16
LOG2E = math.log2(math.e)
epsilon = 1e-06
VMEM = pl.BlockSpec(memory_space=pltpu.VMEM)
SMEM = pl.BlockSpec(memory_space=pltpu.SMEM)
ANY = pl.BlockSpec(memory_space=pl.ANY)
NT = (((1,), (1,)), ((), ()))
TN = (((0,), (0,)), ((), ()))


def mm(a, b, dims=(((1,), (0,)), ((), ()))):
    return lax.dot_general(a, b, dims, preferred_element_type=jnp.float32)


def split(x):
    hi = x.astype(jnp.bfloat16)
    return hi, (x - hi.astype(jnp.float32)).astype(jnp.bfloat16)


def iota(shape, dim):
    return lax.broadcasted_iota(jnp.int32, shape, dim)


def start(copies):
    for one in copies:
        one.start()


def sent(copies):
    for one in copies:
        one.wait_send()


def remote(src, dst, send_sem, recv_sem, **target):
    return pltpu.make_async_remote_copy(
        src_ref=src,
        dst_ref=dst,
        send_sem=send_sem,
        recv_sem=recv_sem,
        device_id=target,
        device_id_type=pl.DeviceIdType.MESH,
    )


def tail_of(total):
    hi, lo = split(total)
    lo, rest = split(total - hi.astype(jnp.float32))
    which = iota((TAIL, total.shape[1]), 0)
    tail = jnp.where(which == 0, hi.astype(jnp.float32), jnp.where(which == 1, lo.astype(jnp.float32), 0.0))
    return jnp.where(which == 2, rest.astype(jnp.float32), tail).astype(jnp.bfloat16)


def layer_kernel(sp, tp, names, *refs):
    m = types.SimpleNamespace(**dict(zip(names, refs)))
    rows, features = m.tok.shape[1:]
    width, wide, narrow = m.wk.shape[1], m.wr.shape[1], m.wi.shape[1]
    heads, rec_heads = width // HEAD, narrow // REC_VAL
    chunks, chunk = m.kv.shape[1], m.kv.shape[3]
    planes = sp // GROUP
    half = planes // 2
    columns = m.out.shape[1]
    span = REC_VAL // GROUP
    me, t = lax.axis_index("sp"), lax.axis_index("tp")
    c, y, z = lax.rem(me, 2), lax.rem(me // 2, 2), me // GROUP
    g = lax.rem(me, GROUP)
    sibling, across = me + 1 - 2 * c, z * GROUP + (1 - y) * 2 + c
    ahead = lax.rem(z + 1, planes) * GROUP + g
    behind = lax.rem(z + planes - 1, planes) * GROUP + g

    def mate(off):
        return z * GROUP + lax.rem(g + off, GROUP)

    def partner(shift):
        return lax.rem(t + shift, tp)

    load_tokens = pltpu.make_async_copy(m.tokens, m.tok.at[t], m.load_sem.at[0])
    load_tokens.start()
    order = "krfivqg"
    loads = [
        pltpu.make_async_copy(getattr(m, "hbm_" + name), getattr(m, "w" + name), m.load_sem.at[1 + i])
        for i, name in enumerate(order)
    ]
    start(loads)
    own_columns = pl.ds(pl.multiple_of(t * columns, columns), columns)
    outer = (m.hbm_attention_out, m.hbm_recurrence_out)
    load_outer = [
        pltpu.make_async_copy(array.at[:, own_columns], m.win.at[t, i], m.load_sem.at[8 + i])
        for i, array in enumerate(outer)
    ]
    start(load_outer)

    barrier = pltpu.get_barrier_semaphore()
    for off in range(1, GROUP):
        pl.semaphore_signal(barrier, inc=1, device_id={"sp": mate(off)}, device_id_type=pl.DeviceIdType.MESH)
    for off in range(1, planes):
        peer = lax.rem(z + off, planes) * GROUP + g
        pl.semaphore_signal(barrier, inc=1, device_id={"sp": peer}, device_id_type=pl.DeviceIdType.MESH)
    for shift in range(1, tp):
        pl.semaphore_signal(barrier, inc=1, device_id={"tp": partner(shift)}, device_id_type=pl.DeviceIdType.MESH)
    pl.semaphore_wait(barrier, GROUP + planes + tp - 3)
    load_tokens.wait()

    def token_copy(shift, r, slot):
        part = m.tok.at[slot, pl.ds(r * chunk, chunk)]
        return remote(part, part, m.tok_send.at[shift, r], m.tok_recv.at[shift, r], tp=partner(shift))

    token_sends = [token_copy(shift, r, t) for shift in range(1, tp) for r in range(chunks)]
    start(token_sends)

    def scale(slot, part):
        value = m.tok[slot, part, :].astype(jnp.float32)
        gains = m.gain[:, pl.ds(pl.multiple_of(slot * features, features), features)]
        return (value * gains).astype(jnp.bfloat16), jnp.sum(value * value, axis=1, keepdims=True)

    def weight_rows(name, slot, cut):
        return getattr(m, "w" + name)[pl.ds(pl.multiple_of(slot * features, features), features), cut]

    def tiles(name):
        size = getattr(m, "w" + name).shape[1]
        step = min(256, size)
        return [slice(i, i + step) for i in range(0, size, step)]

    scaled, squares = scale(t, slice(0, rows))
    m.own_scaled[...] = scaled
    m.square[...] = jnp.broadcast_to(squares, m.square.shape)
    for load, name in zip(loads, order):
        load.wait()
        for cut in tiles(name):
            getattr(m, "a" + name)[:, cut] = mm(m.own_scaled[...], weight_rows(name, t, cut))

    def kv_copy(number, r, way, target):
        piece = m.kv.at[number, r]
        return remote(piece, piece, m.kv_send.at[way, number, r], m.kv_recv.at[number, r], sp=target)

    def relay(zs, ys, r, act):
        number = zs * GROUP + ys * 2 + c
        column, first = ys == y, zs == 0
        here = zs == z

        @pl.when((first & (z + 1 < half)) | (~first & column & (z < planes - 1)))
        def _():
            act(kv_copy(number, r, 0, ahead))

        @pl.when(column & ((here & ((y == 0) | (z == 0))) | (~here & ~first)))
        def _():
            act(kv_copy(number, r, 1, across))

        @pl.when(first & ((z == 0) | (z > half)))
        def _():
            act(kv_copy(number, r, 2, behind))

        @pl.when(~here | (column & (c == 0)) | (~column & (y == 1)))
        def _():
            act(kv_copy(number, r, 3, sibling))

    def event(zs, ys):
        for r in range(chunks):
            kv_copy(zs * GROUP + ys * 2 + c, r, 0, ahead).wait_recv()
            relay(zs, ys, r, lambda one: one.start())

    def from_sibling(zs, ys):
        for r in range(chunks):
            kv_copy(zs * GROUP + ys * 2 + 1 - c, r, 3, sibling).wait_recv()

    for shift in range(1, tp):
        slot = lax.rem(t + tp - shift, tp)
        for r in range(chunks):
            part = slice(r * chunk, (r + 1) * chunk)
            token_copy(shift, r, slot).wait_recv()
            scaled, squares = scale(slot, part)
            m.far_scaled[part] = scaled
            m.square[part] += jnp.broadcast_to(squares, (chunk, LANES))
            if shift == tp - 1:
                inverse = lax.rsqrt(m.square[part, 0:1] * (1.0 / (features * tp)) + epsilon)
                for i, name in enumerate("kv"):
                    whole = getattr(m, "a" + name)[part, :] + mm(
                        m.far_scaled[part], weight_rows(name, slot, slice(0, width))
                    )
                    m.kv[me, r, i * width : (i + 1) * width, :] = (whole * inverse).T.astype(jnp.bfloat16)
                relay(z, y, r, lambda one: one.start())
        if shift < tp - 1:
            for name in order:
                for cut in tiles(name):
                    getattr(m, "a" + name)[:, cut] += mm(m.far_scaled[...], weight_rows(name, slot, cut))
    slot = lax.rem(t + 1, tp)

    def outer_copy(shift, array, other):
        from_columns = array.at[:, pl.ds(pl.multiple_of(partner(shift) * columns, columns), columns)]
        return remote(
            from_columns, m.win.at[t, other], m.outer_send.at[shift, 0], m.outer_recv.at[shift, 0], tp=partner(shift)
        )

    for which, array in enumerate(outer):

        @pl.when(c == which)
        def _():
            start([outer_copy(shift, array, which) for shift in range(1, tp)])

    def outer_share(shift):
        piece = m.win.at[lax.rem(t + tp - shift, tp), c]
        return remote(piece, piece, m.outer_send.at[shift, 1], m.outer_recv.at[shift, 1], sp=sibling)

    inverse = lax.rsqrt(m.square[:, 0:1] * (1.0 / (features * tp)) + epsilon)

    def project(name, cut):
        whole = getattr(m, "a" + name)[:, cut] + mm(m.far_scaled[...], weight_rows(name, slot, cut))
        return (whole * inverse).astype(jnp.bfloat16)

    for name in "rfi":
        for cut in tiles(name):
            getattr(m, "p" + name)[:, cut] = project(name, cut)

    r_iota, c_iota = iota((rows, rows), 0), iota((rows, rows), 1)
    causal = r_iota >= c_iota
    lower = causal.astype(jnp.bfloat16)
    upper = (r_iota <= c_iota).astype(jnp.bfloat16)
    hi, lo = split(m.spike[...])
    spike_col = mm(lower, hi) + mm(lower, lo)
    hi, lo = split(m.spike_t[...])
    spike_row = mm(hi, upper) + mm(lo, upper)
    for h in range(rec_heads):
        ks = slice(h * REC_KEY, (h + 1) * REC_KEY)
        vs = slice(h * REC_VAL, (h + 1) * REC_VAL)
        q = m.pr[:, ks].astype(jnp.float32)
        lifted = q * jax.nn.sigmoid(q)
        intake = (1.0 - m.low[h : h + 1, :]) * jax.nn.sigmoid(-m.pf[:, ks].astype(jnp.float32))
        hi, lo = split(jnp.log1p(-intake))
        run = mm(lower, hi) + mm(lower, lo)
        s_col = spike_col[:, h : h + 1]
        s_row = spike_row[h : h + 1, :]
        q_up = lifted * jnp.exp(run)
        k_down = (intake * jnp.exp(-run)).astype(jnp.bfloat16)
        decay = jnp.exp(jnp.where(causal, s_col - s_row, 0.0))
        inner = jnp.where(causal, mm(q_up.astype(jnp.bfloat16), k_down, NT) * decay, 0.0)
        v = m.pi[:, vs]
        m.local_out[:, vs] = mm(inner.astype(jnp.bfloat16), v)
        m.qdec[:, ks] = (q_up * jnp.exp(s_col)).astype(jnp.bfloat16)
        total = run[rows - 1 : rows, :] + s_col[rows - 1 : rows, :]
        k_end = (intake * jnp.exp(total - (run + s_col))).astype(jnp.bfloat16)
        state = mm(v, k_end, TN).astype(jnp.bfloat16)
        tail = tail_of(total)
        for i in range(GROUP):
            m.s_own[i, 0:span, ks] = state[i * span : (i + 1) * span]
            m.s_own[i, span:, ks] = tail

    def s_copy(off):
        return remote(
            m.s_own.at[lax.rem(g + off, GROUP)], m.s_mates.at[g], m.s_send.at[off], m.s_recv.at[off], sp=mate(off)
        )

    def p_copy(plane):
        return remote(m.p_own, m.p_planes.at[z], m.p_send.at[plane], m.p_recv.at[z], sp=plane * GROUP + g)

    def p_arrival(plane):
        return remote(m.p_own, m.p_planes.at[plane], m.p_send.at[plane], m.p_recv.at[plane], sp=behind)

    def i_copy(off):
        return remote(
            m.i_own.at[lax.rem(g + off, GROUP)], m.i_mates.at[g], m.i_send.at[off], m.i_recv.at[off], sp=mate(off)
        )

    start([s_copy(off) for off in range(1, GROUP)])
    m.s_mates[g] = m.s_own[g]

    for name, place in (("q", None), ("g", m.pg)):
        for cut in tiles(name):
            done = project(name, cut)
            if place is not None:
                place[:, cut] = done
            else:
                for h in range(heads):
                    if cut.start <= h * HEAD < cut.stop:
                        m.qh[h] = done[:, h * HEAD - cut.start : (h + 1) * HEAD - cut.start]

    def parts(packed):
        return packed[0:span].astype(jnp.float32), jnp.sum(packed[span:].astype(jnp.float32), axis=0, keepdims=True)

    def append(state, packed):
        added, total = parts(packed)
        return state * jnp.exp(total) + added

    for off in range(1, GROUP):
        s_copy(off).wait_recv()
    state, total = parts(m.s_mates[0])
    for i in range(1, GROUP):
        state = append(state, m.s_mates[i])
        total = total + parts(m.s_mates[i])[1]
    m.p_own[0:span] = state.astype(jnp.bfloat16)
    m.p_own[span:] = tail_of(total)

    @pl.loop(z + 1, planes)
    def _(plane):
        p_copy(plane).start()

    sums = jnp.where(r_iota > c_iota, -1.0, 0.0).astype(jnp.bfloat16)
    before = c_iota < r_iota

    def attend(numbers, first):
        scores, stays = [], []
        for number in numbers:
            for h in range(heads):
                hs = slice(h * HEAD, (h + 1) * HEAD)
                k = jnp.concatenate([m.kv[number, r, hs, :] for r in range(chunks)], axis=1)
                s = mm(m.qh[h], k) * (HEAD**-0.5 * LOG2E) + m.bias[h] * LOG2E
                soft = jnp.maximum(s, jnp.log2(1.0 + jnp.exp2(jnp.minimum(s, 100.0))))
                scores.append(s - soft)
                stays.append(jnp.where(before, soft, 0.0) if first else soft)
        for i, (score, stay) in enumerate(zip(scores, stays)):
            number, h = numbers[i // heads], i % heads
            vs = slice(width + h * HEAD, width + (h + 1) * HEAD)
            v = jnp.concatenate([m.kv[number, r, vs, :] for r in range(chunks)], axis=1)
            later = mm(stay.astype(jnp.bfloat16), sums)
            w = jnp.exp2(score + later)
            if first:
                w = jnp.where(before, w, 0.0)
            o = mm(w.astype(jnp.bfloat16), v, NT)
            every = jnp.broadcast_to((later - stay)[:, 0:1], (rows, HEAD))
            if first:
                m.acc[h] = o
                m.carry[h] = every
            else:
                m.acc[h] += o * jnp.exp2(m.carry[h])
                m.carry[h] += every

    attend([me], True)

    @pl.when(c == 1)
    def _():
        from_sibling(z, y)
        attend([me - 1], False)

    @pl.loop(0, z)
    def _(plane):
        p_arrival(plane).wait_recv()

    state = lax.fori_loop(
        0, z, lambda plane, so_far: append(so_far, m.p_planes[plane]), jnp.zeros((span, wide), jnp.float32)
    )
    for i in range(GROUP):
        m.i_own[i] = state.astype(jnp.bfloat16)
        state = append(state, m.s_mates[i])
    start([i_copy(off) for off in range(1, GROUP)])
    m.i_mates[g] = m.i_own[g]

    @pl.when((z == 0) & (y == 0))
    def _():
        event(0, 1)

    early = (z == planes - 1) & (z > 1)

    @pl.loop(2 - y, 2 * z + 2)
    def _(step):
        d, ys = step // 2, 1 - lax.rem(step, 2)
        zs = z - d

        @pl.when((ys == 1) & (d > 0) & ~(early & (zs == 0)))
        def _():
            event(zs, y)

        @pl.when((ys != y) & ~(early & (zs == 0)))
        def _():
            event(zs, 1 - y)

        @pl.when(early & (d == 1) & (ys == 1))
        def _():
            event(0, y)

        @pl.when(early & (d == 2) & (ys == 1))
        def _():
            event(0, 1 - y)

        from_sibling(zs, ys)
        attend([zs * GROUP + ys * 2 + 1, zs * GROUP + ys * 2], False)

    for off in range(1, GROUP):
        i_copy(off).wait_recv()
    for h in range(rec_heads):
        ks = slice(h * REC_KEY, (h + 1) * REC_KEY)
        vs = slice(h * REC_VAL, (h + 1) * REC_VAL)
        entering = jnp.concatenate([m.i_mates[i, :, ks] for i in range(GROUP)], axis=0)
        raw = m.local_out[:, vs] + mm(m.qdec[:, ks], entering, NT)
        gate = m.pg[:, vs].astype(jnp.float32)
        mean = jnp.sum(raw * raw, axis=1, keepdims=True) * (1.0 / REC_VAL)
        done = raw * lax.rsqrt(mean + epsilon) * m.norm[...] * (gate * jax.nn.sigmoid(gate))
        m.rec[t, :, vs] = done.astype(jnp.bfloat16)

    def head_copy(i, shift):
        piece = (m.att, m.rec)[i].at[t]
        return remote(piece, piece, m.head_send.at[i, shift], m.head_recv.at[i, shift], tp=partner(shift))

    start([head_copy(1, shift) for shift in range(1, tp)])
    m.att[t] = jnp.concatenate([m.acc[h] for h in range(heads)], axis=1).astype(jnp.bfloat16)
    start([head_copy(0, shift) for shift in range(1, tp)])
    for one in load_outer:
        one.wait()
    mixed = mm(m.att[t], m.win[t, 0]) + mm(m.rec[t], m.win[t, 1])
    for shift in range(1, tp):
        slot = lax.rem(t + tp - shift, tp)
        outer_copy(shift, outer[0], 0).wait_recv()
        outer_share(shift).start()
        outer_share(shift).wait_recv()
        for i in (1, 0):
            head_copy(i, shift).wait_recv()
        mixed = mixed + mm(m.rec[slot], m.win[slot, 1]) + mm(m.att[slot], m.win[slot, 0])
    m.out[...] = mixed.astype(jnp.bfloat16)

    sent(token_sends)
    sent([s_copy(off) for off in range(1, GROUP)] + [i_copy(off) for off in range(1, GROUP)])
    sent([head_copy(i, shift) for i in (0, 1) for shift in range(1, tp)])
    sent([outer_share(shift) for shift in range(1, tp)] + [outer_copy(shift, outer[0], 0) for shift in range(1, tp)])

    @pl.loop(z + 1, planes)
    def _(plane):
        p_copy(plane).wait_send()

    @pl.loop(0, z + 1)
    def _(zs):
        for r in range(chunks):
            relay(zs, y, r, lambda one: one.wait_send())

            @pl.when((zs < z) | (y == 1) | (z == 0))
            def _():
                relay(zs, 1 - y, r, lambda one: one.wait_send())


def shards(sp, tp, *arrays):
    (tokens, gain, wq, wk, wv, bias, wr, wf, wi, wg, low, spike, norm, attention_out, recurrence_out) = arrays
    rows, features = tokens.shape
    width, wide, narrow = wq.shape[1], wr.shape[1], wi.shape[1]
    heads = width // HEAD
    columns = attention_out.shape[1] // tp
    chunk = min(LANES, rows)
    chunks = rows // chunk
    planes = sp // GROUP
    bf16, f32, dma = jnp.bfloat16, jnp.float32, pltpu.SemaphoreType.DMA
    inputs = dict(
        tokens=tokens,
        gain=gain.reshape(1, -1),
        hbm_k=wk,
        hbm_v=wv,
        hbm_q=wq,
        hbm_r=wr,
        hbm_f=wf,
        hbm_i=wi,
        hbm_g=wg,
        bias=bias,
        low=low,
        spike=spike,
        spike_t=spike.T,
        norm=norm.reshape(1, -1),
        hbm_attention_out=attention_out,
        hbm_recurrence_out=recurrence_out,
    )
    in_hbm = [name == "tokens" or name.startswith("hbm") for name in inputs]
    specs = [SMEM if name == "bias" else ANY if hbm else VMEM for name, hbm in zip(inputs, in_hbm)]
    scratch = dict(tok=pltpu.VMEM((tp, rows, features), bf16))
    sizes = dict(k=width, v=width, q=width, r=wide, f=wide, i=narrow, g=narrow)
    for name, size in sizes.items():
        scratch["w" + name] = pltpu.VMEM((features * tp, size), bf16)
        scratch["a" + name] = pltpu.VMEM((rows, size), f32)
        if name in "rfig":
            scratch["p" + name] = pltpu.VMEM((rows, size), bf16)
    scratch.update(
        own_scaled=pltpu.VMEM((rows, features), bf16),
        far_scaled=pltpu.VMEM((rows, features), bf16),
        square=pltpu.VMEM((rows, LANES), f32),
        kv=pltpu.VMEM((sp, chunks, 2 * width, chunk), bf16),
        qh=pltpu.VMEM((heads, rows, HEAD), bf16),
        acc=pltpu.VMEM((heads, rows, HEAD), f32),
        carry=pltpu.VMEM((heads, rows, HEAD), f32),
        local_out=pltpu.VMEM((rows, narrow), f32),
        qdec=pltpu.VMEM((rows, wide), bf16),
        s_own=pltpu.VMEM((GROUP, REC_VAL // GROUP + TAIL, wide), bf16),
        s_mates=pltpu.VMEM((GROUP, REC_VAL // GROUP + TAIL, wide), bf16),
        p_own=pltpu.VMEM((REC_VAL // GROUP + TAIL, wide), bf16),
        p_planes=pltpu.VMEM((planes, REC_VAL // GROUP + TAIL, wide), bf16),
        i_own=pltpu.VMEM((GROUP, REC_VAL // GROUP, wide), bf16),
        i_mates=pltpu.VMEM((GROUP, REC_VAL // GROUP, wide), bf16),
        win=pltpu.VMEM((tp, 2, width, columns), bf16),
        att=pltpu.VMEM((tp, rows, width), bf16),
        rec=pltpu.VMEM((tp, rows, narrow), bf16),
        load_sem=dma((10,)),
        tok_send=dma((tp, chunks)),
        tok_recv=dma((tp, chunks)),
        kv_send=dma((4, sp, chunks)),
        kv_recv=dma((sp, chunks)),
        s_send=dma((GROUP,)),
        s_recv=dma((GROUP,)),
        p_send=dma((planes,)),
        p_recv=dma((planes,)),
        i_send=dma((GROUP,)),
        i_recv=dma((GROUP,)),
        outer_send=dma((tp, 2)),
        outer_recv=dma((tp, 2)),
        head_send=dma((2, tp)),
        head_recv=dma((2, tp)),
    )
    return pl.pallas_call(
        functools.partial(layer_kernel, sp, tp, list(inputs) + ["out"] + list(scratch)),
        out_shape=jax.ShapeDtypeStruct((rows, columns), bf16),
        in_specs=specs,
        out_specs=VMEM,
        scratch_shapes=list(scratch.values()),
        compiler_params=pltpu.CompilerParams(
            collective_id=0, has_side_effects=True, vmem_limit_bytes=60 * 1024 * 1024
        ),
        name="layer",
    )(*inputs.values())


def solution(mesh):
    placed = (
        P("sp", "tp"),
        P(),
        P(None, "tp"),
        P(None, "tp"),
        P(None, "tp"),
        P("tp"),
        P(None, "tp"),
        P(None, "tp"),
        P(None, "tp"),
        P(None, "tp"),
        P("tp", None),
        P("sp", "tp"),
        P(),
        P("tp", None),
        P("tp", None),
    )
    return jax.shard_map(
        functools.partial(shards, mesh.shape["sp"], mesh.shape["tp"]),
        mesh=mesh,
        in_specs=placed,
        out_specs=P("sp", "tp"),
        check_vma=False,
    )
```

```python
import functools
import math
import types

import jax
import jax.numpy as jnp
from jax import lax
from jax.experimental import pallas as pl
from jax.experimental.pallas import tpu as pltpu
from jax.sharding import PartitionSpec as P

HEAD = 64
REC_KEY = 128
REC_VAL = 64
LANES = 128
GROUP = 4
TAIL = 16
LOG2E = math.log2(math.e)
epsilon = 1e-06
VMEM = pl.BlockSpec(memory_space=pltpu.VMEM)
SMEM = pl.BlockSpec(memory_space=pltpu.SMEM)
ANY = pl.BlockSpec(memory_space=pl.ANY)
NT = (((1,), (1,)), ((), ()))
TN = (((0,), (0,)), ((), ()))


def mm(a, b, dims=(((1,), (0,)), ((), ()))):
    return lax.dot_general(a, b, dims, preferred_element_type=jnp.float32)


def split(x):
    hi = x.astype(jnp.bfloat16)
    return hi, (x - hi.astype(jnp.float32)).astype(jnp.bfloat16)


def iota(shape, dim):
    return lax.broadcasted_iota(jnp.int32, shape, dim)


def start(copies):
    for one in copies:
        one.start()


def sent(copies):
    for one in copies:
        one.wait_send()


def remote(src, dst, send_sem, recv_sem, **target):
    return pltpu.make_async_remote_copy(
        src_ref=src,
        dst_ref=dst,
        send_sem=send_sem,
        recv_sem=recv_sem,
        device_id=target,
        device_id_type=pl.DeviceIdType.MESH,
    )


def tail_of(total):
    hi, lo = split(total)
    lo, rest = split(total - hi.astype(jnp.float32))
    which = iota((TAIL, total.shape[1]), 0)
    tail = jnp.where(which == 0, hi.astype(jnp.float32), jnp.where(which == 1, lo.astype(jnp.float32), 0.0))
    return jnp.where(which == 2, rest.astype(jnp.float32), tail).astype(jnp.bfloat16)


def layer_kernel(sp, tp, names, *refs):
    m = types.SimpleNamespace(**dict(zip(names, refs)))
    rows, features = m.tok.shape[1:]
    width, wide, narrow = m.wk.shape[1], m.wr.shape[1], m.wi.shape[1]
    heads, rec_heads = width // HEAD, narrow // REC_VAL
    chunks, chunk = m.kv.shape[1], m.kv.shape[3]
    planes = sp // GROUP
    lend = planes > 2
    columns = m.out.shape[1]
    span = REC_VAL // GROUP
    me, t = lax.axis_index("sp"), lax.axis_index("tp")
    c, y, z = lax.rem(me, 2), lax.rem(me // 2, 2), me // GROUP
    g = lax.rem(me, GROUP)
    sibling, across = me + 1 - 2 * c, z * GROUP + (1 - y) * 2 + c
    ahead = lax.rem(z + 1, planes) * GROUP + g
    bottom, top = g, (planes - 1) * GROUP + g
    lends, borrows = lend & (z == 0), lend & (z == planes - 1)

    def mate(off):
        return z * GROUP + lax.rem(g + off, GROUP)

    def partner(shift):
        return lax.rem(t + shift, tp)

    load_tokens = pltpu.make_async_copy(m.tokens, m.tok.at[t], m.load_sem.at[0])
    load_tokens.start()
    order = "krfivqg"
    loads = [
        pltpu.make_async_copy(getattr(m, "hbm_" + name), getattr(m, "w" + name), m.load_sem.at[1 + i])
        for i, name in enumerate(order)
    ]
    start(loads)
    own_columns = pl.ds(pl.multiple_of(t * columns, columns), columns)
    outer = (m.hbm_attention_out, m.hbm_recurrence_out)
    load_outer = [
        pltpu.make_async_copy(array.at[:, own_columns], m.win.at[t, i], m.load_sem.at[8 + i])
        for i, array in enumerate(outer)
    ]
    start(load_outer)

    barrier = pltpu.get_barrier_semaphore()
    for off in range(1, GROUP):
        pl.semaphore_signal(barrier, inc=1, device_id={"sp": mate(off)}, device_id_type=pl.DeviceIdType.MESH)
    for off in range(1, planes):
        peer = lax.rem(z + off, planes) * GROUP + g
        pl.semaphore_signal(barrier, inc=1, device_id={"sp": peer}, device_id_type=pl.DeviceIdType.MESH)
    for shift in range(1, tp):
        pl.semaphore_signal(barrier, inc=1, device_id={"tp": partner(shift)}, device_id_type=pl.DeviceIdType.MESH)
    pl.semaphore_wait(barrier, GROUP + planes + tp - 3)
    load_tokens.wait()

    def token_copy(shift, r, slot):
        part = m.tok.at[slot, pl.ds(r * chunk, chunk)]
        return remote(part, part, m.tok_send.at[shift, r], m.tok_recv.at[shift, r], tp=partner(shift))

    token_sends = [token_copy(shift, r, t) for shift in range(1, tp) for r in range(chunks)]
    start(token_sends)

    def scale(slot, part):
        value = m.tok[slot, part, :].astype(jnp.float32)
        gains = m.gain[:, pl.ds(pl.multiple_of(slot * features, features), features)]
        return (value * gains).astype(jnp.bfloat16), jnp.sum(value * value, axis=1, keepdims=True)

    def weight_rows(name, slot, cut):
        return getattr(m, "w" + name)[pl.ds(pl.multiple_of(slot * features, features), features), cut]

    def tiles(name):
        size = getattr(m, "w" + name).shape[1]
        step = min(256, size)
        return [slice(i, i + step) for i in range(0, size, step)]

    scaled, squares = scale(t, slice(0, rows))
    m.own_scaled[...] = scaled
    m.square[...] = jnp.broadcast_to(squares, m.square.shape)
    for load, name in zip(loads, order):
        load.wait()
        for cut in tiles(name):
            getattr(m, "a" + name)[:, cut] = mm(m.own_scaled[...], weight_rows(name, t, cut))

    def kv_copy(number, r, way, target):
        piece = m.kv.at[number, r]
        return remote(piece, piece, m.kv_send.at[way, number, r], m.kv_recv.at[number, r], sp=target)

    def relay(zs, ys, r, act):
        number = zs * GROUP + ys * 2 + c
        column, here = ys == y, zs == z
        last = jnp.where(zs == 0, planes - 1 - lend, planes - 1)

        @pl.when(column & (z < last))
        def _():
            act(kv_copy(number, r, 0, ahead))

        @pl.when(column & (~here | (y == 0) | lends))
        def _():
            act(kv_copy(number, r, 1, across))

        @pl.when(~here | (column & (c == 0)) | (~column & (y == 1)) | lends)
        def _():
            act(kv_copy(number, r, 2, sibling))

    def event(cond, zs, ys, r):
        @pl.when(cond & ~(borrows & (zs == 0)))
        def _():
            kv_copy(zs * GROUP + ys * 2 + c, r, 0, ahead).wait_recv()
            relay(zs, ys, r, lambda one: one.start())

    def facing(w):
        return (w <= z + 1) & ((w > 1) | (y == 1) | lends)

    def wave_events(w, r):
        event(w <= z, z - w, y, r)
        event(facing(w), z - w + 1, 1 - y, r)

    def from_sibling(zs, ys):
        for r in range(chunks):
            kv_copy(zs * GROUP + ys * 2 + 1 - c, r, 2, sibling).wait_recv()

    for shift in range(1, tp):
        slot = lax.rem(t + tp - shift, tp)
        for r in range(chunks):
            part = slice(r * chunk, (r + 1) * chunk)
            token_copy(shift, r, slot).wait_recv()
            scaled, squares = scale(slot, part)
            m.far_scaled[part] = scaled
            m.square[part] += jnp.broadcast_to(squares, (chunk, LANES))
            if shift == tp - 1:
                inverse = lax.rsqrt(m.square[part, 0:1] * (1.0 / (features * tp)) + epsilon)
                for i, name in enumerate("kv"):
                    whole = getattr(m, "a" + name)[part, :] + mm(
                        m.far_scaled[part], weight_rows(name, slot, slice(0, width))
                    )
                    m.kv[me, r, i * width : (i + 1) * width, :] = (whole * inverse).T.astype(jnp.bfloat16)
                relay(z, y, r, lambda one: one.start())
        if shift < tp - 1:
            for name in order:
                for cut in tiles(name):
                    getattr(m, "a" + name)[:, cut] += mm(m.far_scaled[...], weight_rows(name, slot, cut))
    slot = lax.rem(t + 1, tp)
    wave_events(1, 0)

    def outer_copy(shift, array, other):
        from_columns = array.at[:, pl.ds(pl.multiple_of(partner(shift) * columns, columns), columns)]
        return remote(
            from_columns, m.win.at[t, other], m.outer_send.at[shift, 0], m.outer_recv.at[shift, 0], tp=partner(shift)
        )

    for which, array in enumerate(outer):

        @pl.when(c == which)
        def _():
            start([outer_copy(shift, array, which) for shift in range(1, tp)])

    def outer_share(shift):
        piece = m.win.at[lax.rem(t + tp - shift, tp), c]
        return remote(piece, piece, m.outer_send.at[shift, 1], m.outer_recv.at[shift, 1], sp=sibling)

    inverse = lax.rsqrt(m.square[:, 0:1] * (1.0 / (features * tp)) + epsilon)

    def project(name, cut):
        whole = getattr(m, "a" + name)[:, cut] + mm(m.far_scaled[...], weight_rows(name, slot, cut))
        return (whole * inverse).astype(jnp.bfloat16)

    def query_copy():
        return remote(m.pq, m.far_q, m.lend_send.at[0], m.lend_recv.at[0], sp=bottom)

    def lent_copy():
        return remote(m.lent, m.lent_back, m.lend_send.at[1], m.lend_recv.at[1], sp=top)

    for name in "qrfig":
        for cut in tiles(name):
            getattr(m, "p" + name)[:, cut] = project(name, cut)
        if name == "q":

            @pl.when(borrows)
            def _():
                query_copy().start()

    r_iota, c_iota = iota((rows, rows), 0), iota((rows, rows), 1)
    causal = r_iota >= c_iota
    lower = causal.astype(jnp.bfloat16)
    upper = (r_iota <= c_iota).astype(jnp.bfloat16)
    spikes = m.spike_t[...] if rec_heads > 1 else jnp.broadcast_to(m.spike_t[...], (8, rows))
    hi, lo = split(spikes)
    spike_col = mm(lower, hi, NT) + mm(lower, lo, NT)
    spike_row = mm(hi, upper) + mm(lo, upper)
    for h in range(rec_heads):
        ks = slice(h * REC_KEY, (h + 1) * REC_KEY)
        vs = slice(h * REC_VAL, (h + 1) * REC_VAL)
        q = m.pr[:, ks].astype(jnp.float32)
        lifted = q * jax.nn.sigmoid(q)
        intake = (1.0 - m.low[h : h + 1, :]) * jax.nn.sigmoid(-m.pf[:, ks].astype(jnp.float32))
        hi, lo = split(jnp.log1p(-intake))
        run = mm(lower, hi) + mm(lower, lo)
        s_col = spike_col[:, h : h + 1]
        s_row = spike_row[h : h + 1, :]
        q_up = lifted * jnp.exp(run)
        k_down = (intake * jnp.exp(-run)).astype(jnp.bfloat16)
        decay = jnp.exp(jnp.where(causal, s_col - s_row, 0.0))
        inner = jnp.where(causal, mm(q_up.astype(jnp.bfloat16), k_down, NT) * decay, 0.0)
        v = m.pi[:, vs]
        m.local_out[:, vs] = mm(inner.astype(jnp.bfloat16), v)
        m.qdec[:, ks] = (q_up * jnp.exp(s_col)).astype(jnp.bfloat16)
        total = run[rows - 1 : rows, :] + s_col[rows - 1 : rows, :]
        k_end = (intake * jnp.exp(total - (run + s_col))).astype(jnp.bfloat16)
        state = mm(v, k_end, TN).astype(jnp.bfloat16)
        tail = tail_of(total)
        for i in range(GROUP):
            m.s_own[i, 0:span, ks] = state[i * span : (i + 1) * span]
            m.s_own[i, span:, ks] = tail

    def s_copy(off):
        return remote(
            m.s_own.at[lax.rem(g + off, GROUP)], m.s_mates.at[g], m.s_send.at[off], m.s_recv.at[off], sp=mate(off)
        )

    def p_copy(plane):
        return remote(m.p_own, m.p_planes.at[z], m.p_send.at[plane], m.p_recv.at[z], sp=plane * GROUP + g)

    def p_arrival(plane):
        return remote(m.p_own, m.p_planes.at[plane], m.p_send.at[plane], m.p_recv.at[plane], sp=bottom)

    def i_copy(off):
        return remote(
            m.i_own.at[lax.rem(g + off, GROUP)], m.i_mates.at[g], m.i_send.at[off], m.i_recv.at[off], sp=mate(off)
        )

    start([s_copy(off) for off in range(1, GROUP)])
    m.s_mates[g] = m.s_own[g]

    def take_queries(queries):
        for h in range(heads):
            m.qh[h] = queries[:, h * HEAD : (h + 1) * HEAD]

    take_queries(m.pq)

    def parts(packed):
        return packed[0:span].astype(jnp.float32), jnp.sum(packed[span:].astype(jnp.float32), axis=0, keepdims=True)

    def append(state, packed):
        added, total = parts(packed)
        return state * jnp.exp(total) + added

    sums = jnp.where(r_iota > c_iota, -1.0, 0.0).astype(jnp.bfloat16)
    before = c_iota < r_iota

    def attend(numbers, place, first=False, after=False):
        scores, stays = [], []
        for number in numbers:
            for h in range(heads):
                hs = slice(h * HEAD, (h + 1) * HEAD)
                k = jnp.concatenate([m.kv[number, r, hs, :] for r in range(chunks)], axis=1)
                s = mm(m.qh[h], k) * (HEAD**-0.5 * LOG2E) + m.bias[h] * LOG2E
                soft = jnp.maximum(s, jnp.log2(1.0 + jnp.exp2(jnp.minimum(s, 100.0))))
                scores.append(s - soft)
                stays.append(jnp.where(before, soft, 0.0) if first else soft)
        done = {}
        for i, (score, stay) in enumerate(zip(scores, stays)):
            number, h = numbers[i // heads], i % heads
            vs = slice(width + h * HEAD, width + (h + 1) * HEAD)
            v = jnp.concatenate([m.kv[number, r, vs, :] for r in range(chunks)], axis=1)
            later = mm(stay.astype(jnp.bfloat16), sums)
            w = jnp.exp2(score + later)
            if first:
                w = jnp.where(before, w, 0.0)
            o = mm(w.astype(jnp.bfloat16), v, NT)
            every = jnp.broadcast_to((later - stay)[:, 0:1], (rows, HEAD))
            if after:
                done[h] = m.part[place, h], m.carry[place, h]
            if h in done:
                o, every = done[h][0] + o * jnp.exp2(done[h][1]), done[h][1] + every
            done[h] = o, every
            if number is numbers[-1]:
                m.part[place, h], m.carry[place, h] = done[h]

    attend([me], 1 - y, first=True)

    @pl.when(c == 1)
    def _():
        from_sibling(z, y)
        attend([me - 1], 1 - y, after=True)

    def gather_states():
        for off in range(1, GROUP):
            s_copy(off).wait_recv()
        state, total = parts(m.s_mates[0])
        for i in range(1, GROUP):
            state = append(state, m.s_mates[i])
            total = total + parts(m.s_mates[i])[1]
        m.p_own[0:span] = state.astype(jnp.bfloat16)
        m.p_own[span:] = tail_of(total)

        @pl.loop(z + 1, planes)
        def _(plane):
            p_copy(plane).start()

    def enter_states():
        @pl.loop(0, z)
        def _(plane):
            p_arrival(plane).wait_recv()

        state = lax.fori_loop(
            0, z, lambda plane, so_far: append(so_far, m.p_planes[plane]), jnp.zeros((span, wide), jnp.float32)
        )
        for i in range(GROUP):
            m.i_own[i] = state.astype(jnp.bfloat16)
            state = append(state, m.s_mates[i])
        start([i_copy(off) for off in range(1, GROUP)])
        m.i_mates[g] = m.i_own[g]

    def head_copy(i, shift):
        piece = (m.att, m.rec)[i].at[t]
        return remote(piece, piece, m.head_send.at[i, shift], m.head_recv.at[i, shift], tp=partner(shift))

    def finish_states():
        for off in range(1, GROUP):
            i_copy(off).wait_recv()
        for h in range(rec_heads):
            ks = slice(h * REC_KEY, (h + 1) * REC_KEY)
            vs = slice(h * REC_VAL, (h + 1) * REC_VAL)
            entering = jnp.concatenate([m.i_mates[i, :, ks] for i in range(GROUP)], axis=0)
            raw = m.local_out[:, vs] + mm(m.qdec[:, ks], entering, NT)
            gate = m.pg[:, vs].astype(jnp.float32)
            mean = jnp.sum(raw * raw, axis=1, keepdims=True) * (1.0 / REC_VAL)
            done = raw * lax.rsqrt(mean + epsilon) * m.norm[...] * (gate * jax.nn.sigmoid(gate))
            m.rec[t, :, vs] = done.astype(jnp.bfloat16)
        start([head_copy(1, shift) for shift in range(1, tp)])

    @pl.loop(1, z + 2)
    def _(w):
        for r in range(1, chunks):
            wave_events(w, r)

        @pl.when(w == 3)
        def _():
            finish_states()

        @pl.loop(0, 2)
        def _(i):
            zs, ys = z - w + 1 - i, jnp.where(i == 0, 1 - y, y)

            @pl.when((zs >= 0) & ((i == 1) | (w > 1) | (y == 1)) & ~(borrows & (zs == 0)))
            def _():
                from_sibling(zs, ys)
                attend([zs * GROUP + ys * 2 + 1, zs * GROUP + ys * 2], 2 * (z - zs) + 1 - ys)

            @pl.when((w == 2) & (i == 0))
            def _():
                enter_states()

        wave_events(w + 1, 0)

        @pl.when(w == 1)
        def _():
            gather_states()

    @pl.when(z == 0)
    def _():
        enter_states()

    if lend:

        @pl.when(z == 0)
        def _():
            query_copy().wait_recv()
            take_queries(m.far_q)

            @pl.when(c == 0)
            def _():
                from_sibling(0, y)

            @pl.when(y == 0)
            def _():
                from_sibling(0, 1)

            @pl.loop(0, 2)
            def _(i):
                attend([3 - 2 * i, 2 - 2 * i], 2 + i)

            for h in range(heads):
                whole = m.part[2, h] + m.part[3, h] * jnp.exp2(m.carry[2, h])
                m.lent[:, h * HEAD : (h + 1) * HEAD] = whole.astype(jnp.bfloat16)
            lent_copy().start()

    @pl.when(z < 2)
    def _():
        finish_states()

    for shift in range(1, tp):
        outer_copy(shift, outer[0], 0).wait_recv()
        outer_share(shift).start()

    @pl.loop(2 - y, 2 * z + 2 - 2 * borrows.astype(jnp.int32))
    def _(place):
        for h in range(heads):
            m.part[1 - y, h] += m.part[place, h] * jnp.exp2(m.carry[1 - y, h])
            m.carry[1 - y, h] += m.carry[place, h]

    @pl.when(borrows)
    def _():
        lent_copy().wait_recv()
        for h in range(heads):
            lent = m.lent_back[:, h * HEAD : (h + 1) * HEAD].astype(jnp.float32)
            m.part[1 - y, h] += lent * jnp.exp2(m.carry[1 - y, h])

    m.att[t] = jnp.concatenate([m.part[1 - y, h] for h in range(heads)], axis=1).astype(jnp.bfloat16)
    start([head_copy(0, shift) for shift in range(1, tp)])
    for one in load_outer:
        one.wait()
    mixed = mm(m.att[t], m.win[t, 0]) + mm(m.rec[t], m.win[t, 1])
    for shift in range(1, tp):
        slot = lax.rem(t + tp - shift, tp)
        outer_share(shift).wait_recv()
        for i in (1, 0):
            head_copy(i, shift).wait_recv()
        mixed = mixed + mm(m.rec[slot], m.win[slot, 1]) + mm(m.att[slot], m.win[slot, 0])
    m.out[...] = mixed.astype(jnp.bfloat16)

    sent(token_sends)
    sent([s_copy(off) for off in range(1, GROUP)] + [i_copy(off) for off in range(1, GROUP)])
    sent([head_copy(i, shift) for i in (0, 1) for shift in range(1, tp)])
    sent([outer_share(shift) for shift in range(1, tp)] + [outer_copy(shift, outer[0], 0) for shift in range(1, tp)])

    @pl.loop(z + 1, planes)
    def _(plane):
        p_copy(plane).wait_send()

    @pl.loop(borrows.astype(jnp.int32), z + 1)
    def _(zs):
        for r in range(chunks):
            relay(zs, y, r, lambda one: one.wait_send())

            @pl.when((zs < z) | (y == 1) | lends)
            def _():
                relay(zs, 1 - y, r, lambda one: one.wait_send())

    @pl.when(borrows)
    def _():
        query_copy().wait_send()

    @pl.when(lends)
    def _():
        lent_copy().wait_send()


def shards(sp, tp, *arrays):
    (tokens, gain, wq, wk, wv, bias, wr, wf, wi, wg, low, spike, norm, attention_out, recurrence_out) = arrays
    rows, features = tokens.shape
    width, wide, narrow = wq.shape[1], wr.shape[1], wi.shape[1]
    heads = width // HEAD
    columns = attention_out.shape[1] // tp
    chunk = min(LANES, rows)
    chunks = rows // chunk
    planes = sp // GROUP
    bf16, f32, dma = jnp.bfloat16, jnp.float32, pltpu.SemaphoreType.DMA
    inputs = dict(
        tokens=tokens,
        gain=gain.reshape(1, -1),
        hbm_k=wk,
        hbm_v=wv,
        hbm_q=wq,
        hbm_r=wr,
        hbm_f=wf,
        hbm_i=wi,
        hbm_g=wg,
        bias=bias,
        low=low,
        spike_t=spike.T,
        norm=norm.reshape(1, -1),
        hbm_attention_out=attention_out,
        hbm_recurrence_out=recurrence_out,
    )
    in_hbm = [name == "tokens" or name.startswith("hbm") for name in inputs]
    specs = [SMEM if name == "bias" else ANY if hbm else VMEM for name, hbm in zip(inputs, in_hbm)]
    scratch = dict(tok=pltpu.VMEM((tp, rows, features), bf16))
    sizes = dict(k=width, v=width, q=width, r=wide, f=wide, i=narrow, g=narrow)
    for name, size in sizes.items():
        scratch["w" + name] = pltpu.VMEM((features * tp, size), bf16)
        scratch["a" + name] = pltpu.VMEM((rows, size), f32)
        if name in "qrfig":
            scratch["p" + name] = pltpu.VMEM((rows, size), bf16)
    scratch.update(
        own_scaled=pltpu.VMEM((rows, features), bf16),
        far_scaled=pltpu.VMEM((rows, features), bf16),
        square=pltpu.VMEM((rows, LANES), f32),
        kv=pltpu.VMEM((sp, chunks, 2 * width, chunk), bf16),
        qh=pltpu.VMEM((heads, rows, HEAD), bf16),
        part=pltpu.VMEM((max(4, 2 * planes), heads, rows, HEAD), f32),
        carry=pltpu.VMEM((max(4, 2 * planes), heads, rows, HEAD), f32),
        local_out=pltpu.VMEM((rows, narrow), f32),
        qdec=pltpu.VMEM((rows, wide), bf16),
        s_own=pltpu.VMEM((GROUP, REC_VAL // GROUP + TAIL, wide), bf16),
        s_mates=pltpu.VMEM((GROUP, REC_VAL // GROUP + TAIL, wide), bf16),
        p_own=pltpu.VMEM((REC_VAL // GROUP + TAIL, wide), bf16),
        p_planes=pltpu.VMEM((planes, REC_VAL // GROUP + TAIL, wide), bf16),
        i_own=pltpu.VMEM((GROUP, REC_VAL // GROUP, wide), bf16),
        i_mates=pltpu.VMEM((GROUP, REC_VAL // GROUP, wide), bf16),
        win=pltpu.VMEM((tp, 2, width, columns), bf16),
        far_q=pltpu.VMEM((rows, width), bf16),
        lent=pltpu.VMEM((rows, width), bf16),
        lent_back=pltpu.VMEM((rows, width), bf16),
        att=pltpu.VMEM((tp, rows, width), bf16),
        rec=pltpu.VMEM((tp, rows, narrow), bf16),
        load_sem=dma((10,)),
        tok_send=dma((tp, chunks)),
        tok_recv=dma((tp, chunks)),
        kv_send=dma((3, sp, chunks)),
        lend_send=dma((2,)),
        lend_recv=dma((2,)),
        kv_recv=dma((sp, chunks)),
        s_send=dma((GROUP,)),
        s_recv=dma((GROUP,)),
        p_send=dma((planes,)),
        p_recv=dma((planes,)),
        i_send=dma((GROUP,)),
        i_recv=dma((GROUP,)),
        outer_send=dma((tp, 2)),
        outer_recv=dma((tp, 2)),
        head_send=dma((2, tp)),
        head_recv=dma((2, tp)),
    )
    return pl.pallas_call(
        functools.partial(layer_kernel, sp, tp, list(inputs) + ["out"] + list(scratch)),
        out_shape=jax.ShapeDtypeStruct((rows, columns), bf16),
        in_specs=specs,
        out_specs=VMEM,
        scratch_shapes=list(scratch.values()),
        compiler_params=pltpu.CompilerParams(
            collective_id=0, has_side_effects=True, vmem_limit_bytes=60 * 1024 * 1024
        ),
        name="layer",
    )(*inputs.values())


def solution(mesh):
    placed = (
        P("sp", "tp"),
        P(),
        P(None, "tp"),
        P(None, "tp"),
        P(None, "tp"),
        P("tp"),
        P(None, "tp"),
        P(None, "tp"),
        P(None, "tp"),
        P(None, "tp"),
        P("tp", None),
        P("sp", "tp"),
        P(),
        P("tp", None),
        P("tp", None),
    )
    return jax.shard_map(
        functools.partial(shards, mesh.shape["sp"], mesh.shape["tp"]),
        mesh=mesh,
        in_specs=placed,
        out_specs=P("sp", "tp"),
        check_vma=False,
    )
```

```python
import functools
import math
import types

import jax
import jax.numpy as jnp
from jax import lax
from jax.experimental import pallas as pl
from jax.experimental.pallas import tpu as pltpu
from jax.sharding import PartitionSpec as P

HEAD = 64
REC_KEY = 128
REC_VAL = 64
LANES = 128
GROUP = 4
TAIL = 16
CHUNKS = 4
LOG2E = math.log2(math.e)
epsilon = 1e-06
VMEM = pl.BlockSpec(memory_space=pltpu.VMEM)
SMEM = pl.BlockSpec(memory_space=pltpu.SMEM)
ANY = pl.BlockSpec(memory_space=pl.ANY)
NT = (((1,), (1,)), ((), ()))
TN = (((0,), (0,)), ((), ()))


def mm(a, b, dims=(((1,), (0,)), ((), ()))):
    return lax.dot_general(a, b, dims, preferred_element_type=jnp.float32)


def split(x):
    hi = x.astype(jnp.bfloat16)
    return hi, (x - hi.astype(jnp.float32)).astype(jnp.bfloat16)


def iota(shape, dim):
    return lax.broadcasted_iota(jnp.int32, shape, dim)


def start(copies):
    for one in copies:
        one.start()


def sent(copies):
    for one in copies:
        one.wait_send()


def remote(src, dst, send_sem, recv_sem, **target):
    return pltpu.make_async_remote_copy(
        src_ref=src,
        dst_ref=dst,
        send_sem=send_sem,
        recv_sem=recv_sem,
        device_id=target,
        device_id_type=pl.DeviceIdType.MESH,
    )


def tail_of(total):
    hi, lo = split(total)
    lo, rest = split(total - hi.astype(jnp.float32))
    which = iota((TAIL, total.shape[1]), 0)
    tail = jnp.where(which == 0, hi.astype(jnp.float32), jnp.where(which == 1, lo.astype(jnp.float32), 0.0))
    return jnp.where(which == 2, rest.astype(jnp.float32), tail).astype(jnp.bfloat16)


def layer_kernel(sp, tp, names, *refs):
    m = types.SimpleNamespace(**dict(zip(names, refs)))
    rows, features = m.tok.shape[1:]
    width, wide, narrow = m.wk.shape[1], m.wr.shape[1], m.wi.shape[1]
    heads, rec_heads = width // HEAD, narrow // REC_VAL
    chunks, chunk = CHUNKS, rows // CHUNKS
    planes = sp // GROUP
    lend = planes > 2
    columns = m.out.shape[1]
    span = REC_VAL // GROUP
    together = m.att.shape[3] // HEAD
    batches = [range(h, h + together) for h in range(0, heads, together)]
    me, t = lax.axis_index("sp"), lax.axis_index("tp")
    c, y, z = lax.rem(me, 2), lax.rem(me // 2, 2), me // GROUP
    g = lax.rem(me, GROUP)
    sibling, across = me + 1 - 2 * c, z * GROUP + (1 - y) * 2 + c
    ahead = lax.rem(z + 1, planes) * GROUP + g
    bottom, top = g, (planes - 1) * GROUP + g
    lends, borrows = lend & (z == 0), lend & (z == planes - 1)

    def mate(off):
        return z * GROUP + lax.rem(g + off, GROUP)

    def partner(shift):
        return lax.rem(t + shift, tp)

    load_tokens = pltpu.make_async_copy(m.tokens, m.tok.at[t], m.load_sem.at[0])
    load_tokens.start()
    order = "krfivqg"
    loads = [
        pltpu.make_async_copy(getattr(m, "hbm_" + name), getattr(m, "w" + name), m.load_sem.at[1 + i])
        for i, name in enumerate(order)
    ]
    start(loads)
    own_columns = pl.ds(pl.multiple_of(t * columns, columns), columns)
    outer = (m.hbm_attention_out, m.hbm_recurrence_out)
    load_outer = [
        pltpu.make_async_copy(array.at[:, own_columns], m.win.at[t, i], m.load_sem.at[8 + i])
        for i, array in enumerate(outer)
    ]
    start(load_outer)

    barrier = pltpu.get_barrier_semaphore()
    for off in range(1, GROUP):
        pl.semaphore_signal(barrier, inc=1, device_id={"sp": mate(off)}, device_id_type=pl.DeviceIdType.MESH)
    for off in range(1, planes):
        peer = lax.rem(z + off, planes) * GROUP + g
        pl.semaphore_signal(barrier, inc=1, device_id={"sp": peer}, device_id_type=pl.DeviceIdType.MESH)
    for shift in range(1, tp):
        pl.semaphore_signal(barrier, inc=1, device_id={"tp": partner(shift)}, device_id_type=pl.DeviceIdType.MESH)
    pl.semaphore_wait(barrier, GROUP + planes + tp - 3)
    load_tokens.wait()

    def token_copy(shift, r, slot):
        part = m.tok.at[slot, pl.ds(r * chunk, chunk)]
        return remote(part, part, m.tok_send.at[shift - 1], m.tok_recv.at[shift - 1, r], tp=partner(shift))

    token_sends = [token_copy(shift, r, t) for shift in range(1, tp) for r in range(chunks)]
    start(token_sends)

    def scale(slot, part):
        value = m.tok[slot, part, :].astype(jnp.float32)
        gains = m.gain[:, pl.ds(pl.multiple_of(slot * features, features), features)]
        return (value * gains).astype(jnp.bfloat16), jnp.sum(value * value, axis=1, keepdims=True)

    def weight_rows(name, slot, cut):
        return getattr(m, "w" + name)[pl.ds(pl.multiple_of(slot * features, features), features), cut]

    def tiles(name):
        size = getattr(m, "w" + name).shape[1]
        step = min(256, size)
        return [slice(i, i + step) for i in range(0, size, step)]

    scaled, squares = scale(t, slice(0, rows))
    m.own_scaled[...] = scaled
    m.square[...] = jnp.broadcast_to(squares, m.square.shape)
    for load, name in zip(loads, order):
        load.wait()
        for cut in tiles(name):
            getattr(m, "a" + name)[:, cut] = mm(m.own_scaled[...], weight_rows(name, t, cut))

    def kv_copy(number, r, way, target):
        piece = m.kv.at[number, pl.ds(r * chunk, chunk)]
        kind = number // 2
        if way == 2:
            return remote(piece, piece, m.kv_send.at[2, kind], m.sib_recv.at[kind], sp=target)
        return remote(piece, piece, m.kv_send.at[way, kind], m.kv_recv.at[kind, r], sp=target)

    def kv_whole(number, way):
        piece, kind = m.kv.at[number], number // 2
        return remote(piece, piece, m.kv_send.at[way, kind], m.sib_recv.at[kind], sp=sibling)

    def relay(zs, ys, r, act):
        copy = kv_copy if r is not None else lambda number, r, way, target: kv_whole(number, way)
        number = zs * GROUP + ys * 2 + c
        column, here = ys == y, zs == z
        last = jnp.where(zs == 0, planes - 1 - lend, planes - 1)

        @pl.when(column & (z < last))
        def _():
            act(copy(number, r, 0, ahead))

        @pl.when(column & (~here | (y == 0) | lends))
        def _():
            act(copy(number, r, 1, across))

        @pl.when(~here | (column & (c == 0)) | (~column & (y == 1)) | lends)
        def _():
            act(copy(number, r, 2, sibling))

    def event(cond, zs, ys, r):
        @pl.when(cond & ~(borrows & (zs == 0)))
        def _():
            kv_copy(zs * GROUP + ys * 2 + c, r, 0, ahead).wait_recv()
            relay(zs, ys, r, lambda one: one.start())

    def facing(w):
        return (w <= z + 1) & ((w > 1) | (y == 1) | lends)

    def wave_events(w, r):
        event(w <= z, z - w, y, r)
        event(facing(w), z - w + 1, 1 - y, r)

    def from_sibling(zs, ys):
        kv_whole(zs * GROUP + ys * 2 + 1 - c, 2).wait_recv()

    part_rows = rows // 2
    r_iota, c_iota = iota((part_rows, part_rows), 0), iota((part_rows, part_rows), 1)
    causal = r_iota >= c_iota
    lower = causal.astype(jnp.bfloat16)
    upper = (r_iota <= c_iota).astype(jnp.bfloat16)

    def project(name, part):
        inverse = lax.rsqrt(m.square[part, 0:1] * (1.0 / (features * tp)) + epsilon)
        for cut in tiles(name):
            whole = getattr(m, "a" + name)[part, cut] + mm(
                m.far_scaled[part], weight_rows(name, lax.rem(t + 1, tp), cut)
            )
            getattr(m, "p" + name)[part, cut] = (whole * inverse).astype(jnp.bfloat16)

    def recur(which):
        part = slice(which * part_rows, (which + 1) * part_rows)
        spikes = m.spike_t[:, part]
        if rec_heads == 1:
            spikes = jnp.broadcast_to(spikes, (8, part_rows))
        hi, lo = split(spikes)
        spike_col = mm(lower, hi, NT) + mm(lower, lo, NT)
        spike_row = mm(hi, upper) + mm(lo, upper)
        for h in range(rec_heads):
            ks = slice(h * REC_KEY, (h + 1) * REC_KEY)
            vs = slice(h * REC_VAL, (h + 1) * REC_VAL)
            q = m.pr[part, ks].astype(jnp.float32)
            lifted = q * jax.nn.sigmoid(q)
            intake = (1.0 - m.low[h : h + 1, :]) * jax.nn.sigmoid(-m.pf[part, ks].astype(jnp.float32))
            hi, lo = split(jnp.log1p(-intake))
            run = mm(lower, hi) + mm(lower, lo)
            s_col = spike_col[:, h : h + 1]
            s_row = spike_row[h : h + 1, :]
            q_up = lifted * jnp.exp(run)
            k_down = (intake * jnp.exp(-run)).astype(jnp.bfloat16)
            decay = jnp.exp(jnp.where(causal, s_col - s_row, 0.0))
            inner = jnp.where(causal, mm(q_up.astype(jnp.bfloat16), k_down, NT) * decay, 0.0)
            v = m.pi[part, vs]
            output = mm(inner.astype(jnp.bfloat16), v)
            decayed = q_up * jnp.exp(s_col)
            total = run[part_rows - 1 : part_rows, :] + s_col[part_rows - 1 : part_rows, :]
            k_end = (intake * jnp.exp(total - (run + s_col))).astype(jnp.bfloat16)
            state = mm(v, k_end, TN)
            if which == 0:
                m.local_out[part, vs] = output
                m.qdec[part, ks] = decayed.astype(jnp.bfloat16)
                m.half_state[:, ks] = state
                m.half_total[:, ks] = total
                continue
            earlier = m.half_state[:, ks]
            m.local_out[part, vs] = output + mm(decayed.astype(jnp.bfloat16), earlier.astype(jnp.bfloat16), NT)
            m.qdec[part, ks] = (decayed * jnp.exp(m.half_total[:, ks])).astype(jnp.bfloat16)
            state = (earlier * jnp.exp(total) + state).astype(jnp.bfloat16)
            tail = tail_of(total + m.half_total[:, ks])
            for i in range(GROUP):
                m.s_own[i, 0:span, ks] = state[i * span : (i + 1) * span]
                m.s_own[i, span:, ks] = tail

    first_rows, last_rows = slice(0, part_rows), slice(part_rows, rows)

    for shift in range(1, tp):
        slot = lax.rem(t + tp - shift, tp)
        for r in range(chunks):
            part = slice(r * chunk, (r + 1) * chunk)
            token_copy(shift, r, slot).wait_recv()
            scaled, squares = scale(slot, part)
            m.far_scaled[part] = scaled
            m.square[part] += jnp.broadcast_to(squares, (chunk, LANES))
            if shift == tp - 1:
                inverse = lax.rsqrt(m.square[part, 0:1] * (1.0 / (features * tp)) + epsilon)
                for i, name in enumerate("kv"):
                    whole = getattr(m, "a" + name)[part, :] + mm(
                        m.far_scaled[part], weight_rows(name, slot, slice(0, width))
                    )
                    m.kv[me, part, i * width : (i + 1) * width] = (whole * inverse).astype(jnp.bfloat16)
                relay(z, y, r, lambda one: one.start())
                if 0 < r < chunks - 1:
                    wave_events(1, r - 1)
                if r == chunks // 2 - 1:
                    for name in "qrfi":
                        project(name, first_rows)
                    recur(0)
        if shift < tp - 1:
            for name in order:
                for cut in tiles(name):
                    getattr(m, "a" + name)[:, cut] += mm(m.far_scaled[...], weight_rows(name, slot, cut))
    slot = lax.rem(t + 1, tp)
    def outer_copy(shift, array, other):
        from_columns = array.at[:, pl.ds(pl.multiple_of(partner(shift) * columns, columns), columns)]
        return remote(
            from_columns, m.win.at[t, other], m.outer_send.at[shift - 1, 0], m.outer_recv.at[shift - 1, 0], tp=partner(shift)
        )

    for which, array in enumerate(outer):

        @pl.when(c == which)
        def _():
            start([outer_copy(shift, array, which) for shift in range(1, tp)])

    def outer_share(shift):
        piece = m.win.at[lax.rem(t + tp - shift, tp), c]
        return remote(piece, piece, m.outer_send.at[shift - 1, 1], m.outer_recv.at[shift - 1, 1], sp=sibling)

    def query_copy():
        return remote(m.pq, m.far_q, m.lend_send.at[0], m.lend_recv.at[0], sp=bottom)

    def lent_copy():
        return remote(m.lent, m.lent_back, m.lend_send.at[1], m.lend_recv.at[1], sp=top)

    project("q", last_rows)

    @pl.when(borrows)
    def _():
        query_copy().start()

    for name in "rfi":
        project(name, last_rows)
    recur(1)

    def s_copy(off):
        return remote(
            m.s_own.at[lax.rem(g + off, GROUP)], m.s_mates.at[g], m.s_send, m.s_recv.at[off - 1], sp=mate(off)
        )

    def p_copy(plane):
        return remote(m.p_own, m.p_planes.at[z], m.p_send.at[plane], m.p_recv.at[z], sp=plane * GROUP + g)

    def p_arrival(plane):
        return remote(m.p_own, m.p_planes.at[plane], m.p_send.at[plane], m.p_recv.at[plane], sp=bottom)

    def i_copy(off):
        return remote(
            m.i_own.at[lax.rem(g + off, GROUP)], m.i_mates.at[g], m.i_send, m.i_recv.at[off - 1], sp=mate(off)
        )

    start([s_copy(off) for off in range(1, GROUP)])
    project("g", slice(0, rows))
    wave_events(1, chunks - 2)
    wave_events(2, 0)
    m.s_mates[g] = m.s_own[g]

    def take_queries(queries):
        for h in range(heads):
            m.qh[h] = queries[:, h * HEAD : (h + 1) * HEAD]

    take_queries(m.pq)

    def parts(packed):
        return packed[0:span].astype(jnp.float32), jnp.sum(packed[span:].astype(jnp.float32), axis=0, keepdims=True)

    def append(state, packed):
        added, total = parts(packed)
        return state * jnp.exp(total) + added

    r_iota, c_iota = iota((rows, rows), 0), iota((rows, rows), 1)
    sums = jnp.where(r_iota > c_iota, -1.0, 0.0).astype(jnp.bfloat16)
    before = c_iota < r_iota

    def attend(numbers, place, first=False, after=False, some=range(heads)):
        scores, stays = [], []
        for number in numbers:
            for h in some:
                hs = slice(h * HEAD, (h + 1) * HEAD)
                s = mm(m.qh[h], m.kv[number, :, hs], NT) * (HEAD**-0.5 * LOG2E) + m.bias[h] * LOG2E
                soft = jnp.maximum(s, jnp.log2(1.0 + jnp.exp2(jnp.minimum(s, 100.0))))
                scores.append(s - soft)
                stays.append(jnp.where(before, soft, 0.0) if first else soft)
        done = {}
        for i, (score, stay) in enumerate(zip(scores, stays)):
            number, h = numbers[i // len(some)], some[i % len(some)]
            vs = slice(width + h * HEAD, width + (h + 1) * HEAD)
            later = mm(stay.astype(jnp.bfloat16), sums)
            w = jnp.exp2(score + later)
            if first:
                w = jnp.where(before, w, 0.0)
            o = mm(w.astype(jnp.bfloat16), m.kv[number, :, vs])
            every = jnp.broadcast_to((later - stay)[:, 0:1], (rows, HEAD))
            if after:
                done[h] = m.part[place, h], m.carry[place, h]
            if h in done:
                o, every = done[h][0] + o * jnp.exp2(done[h][1]), done[h][1] + every
            done[h] = o, every
            if number is numbers[-1]:
                m.part[place, h], m.carry[place, h] = done[h]

    attend([me], 1 - y, first=True)
    wave_events(1, chunks - 1)
    wave_events(2, 1)

    @pl.when(c == 1)
    def _():
        from_sibling(z, y)
        attend([me - 1], 1 - y, after=True)

    def combine(place, some=range(heads)):
        for h in some:
            m.part[1 - y, h] += m.part[place, h] * jnp.exp2(m.carry[1 - y, h])
            m.carry[1 - y, h] += m.carry[place, h]

    def combine_wave(w):
        for place in (2 * w - 2, 2 * w - 1):

            @pl.when(place > 1 - y)
            def _():
                combine(place)

    def gather_states():
        for off in range(1, GROUP):
            s_copy(off).wait_recv()
        state, total = parts(m.s_mates[0])
        for i in range(1, GROUP):
            state = append(state, m.s_mates[i])
            total = total + parts(m.s_mates[i])[1]
        m.p_own[0:span] = state.astype(jnp.bfloat16)
        m.p_own[span:] = tail_of(total)

        @pl.loop(z + 1, planes)
        def _(plane):
            p_copy(plane).start()

    def enter_states():
        @pl.loop(0, z)
        def _(plane):
            p_arrival(plane).wait_recv()

        state = lax.fori_loop(
            0, z, lambda plane, so_far: append(so_far, m.p_planes[plane]), jnp.zeros((span, wide), jnp.float32)
        )
        for i in range(GROUP):
            m.i_own[i] = state.astype(jnp.bfloat16)
            state = append(state, m.s_mates[i])
        start([i_copy(off) for off in range(1, GROUP)])
        m.i_mates[g] = m.i_own[g]

    def head_copy(i, shift):
        piece = m.rec.at[t] if i == len(batches) else m.att.at[t, i]
        return remote(piece, piece, m.head_send.at[i, shift - 1], m.head_recv.at[i, shift - 1], tp=partner(shift))

    def finish_states():
        for off in range(1, GROUP):
            i_copy(off).wait_recv()
        for h in range(rec_heads):
            ks = slice(h * REC_KEY, (h + 1) * REC_KEY)
            vs = slice(h * REC_VAL, (h + 1) * REC_VAL)
            entering = jnp.concatenate([m.i_mates[i, :, ks] for i in range(GROUP)], axis=0)
            raw = m.local_out[:, vs] + mm(m.qdec[:, ks], entering, NT)
            gate = m.pg[:, vs].astype(jnp.float32)
            mean = jnp.sum(raw * raw, axis=1, keepdims=True) * (1.0 / REC_VAL)
            done = raw * lax.rsqrt(mean + epsilon) * m.norm[...] * (gate * jax.nn.sigmoid(gate))
            m.rec[t, :, vs] = done.astype(jnp.bfloat16)
        start([head_copy(len(batches), shift) for shift in range(1, tp)])

    waves = z + 1 - borrows.astype(jnp.int32)

    @pl.loop(1, waves + 1)
    def _(w):
        @pl.when(w > 1)
        def _():
            combine_wave(w - 1)
            wave_events(w, chunks - 1)

        @pl.when(w == 3)
        def _():
            finish_states()

        @pl.loop(0, 2)
        def _(i):
            zs, ys = z - w + 1 - i, jnp.where(i == 0, 1 - y, y)

            @pl.when((i == 1) & (zs >= 0) & ~(borrows & (zs == 0)) | (i == 0) & ((w > 1) | (y == 1)) & (w < waves))
            def _():
                from_sibling(zs, ys)
                attend([zs * GROUP + ys * 2 + 1, zs * GROUP + ys * 2], 2 * (z - zs) + 1 - ys)

            @pl.when((w == 1) & (i == 0))
            def _():
                for r in range(2, chunks - 1):
                    wave_events(2, r)

            @pl.when((w > 1) & (i == 0))
            def _():
                for r in range(chunks - 1):
                    wave_events(w + 1, r)

            @pl.when((w == 2) & (i == 0))
            def _():
                enter_states()

        @pl.when(w == 1)
        def _():
            gather_states()

    @pl.when(z == 0)
    def _():
        enter_states()

    if lend:

        @pl.when(z == 0)
        def _():
            query_copy().wait_recv()
            take_queries(m.far_q)

            @pl.when(c == 0)
            def _():
                from_sibling(0, y)

            from_sibling(0, 1 - y)

            @pl.loop(0, 2)
            def _(i):
                attend([3 - 2 * i, 2 - 2 * i], 2 + i)

            for h in range(heads):
                whole = m.part[2, h] + m.part[3, h] * jnp.exp2(m.carry[2, h])
                m.lent[:, h * HEAD : (h + 1) * HEAD] = whole.astype(jnp.bfloat16)
            lent_copy().start()
            take_queries(m.pq)

    @pl.when(z < 2)
    def _():
        finish_states()

    for shift in range(1, tp):
        outer_copy(shift, outer[0], 0).wait_recv()
        outer_share(shift).start()
    for one in load_outer:
        one.wait()

    end, last = waves - 1, z - waves + 1
    facing_end = (waves > 1) | (y == 1)

    @pl.when(facing_end & ~lends)
    def _():
        from_sibling(last, 1 - y)

    @pl.when(borrows)
    def _():
        lent_copy().wait_recv()

    for j, some in enumerate(batches):

        @pl.when(facing_end)
        def _():
            attend([last * GROUP + (1 - y) * 2 + 1, last * GROUP + (1 - y) * 2], 2 * end + y, some=some)

        for place in (2 * end, 2 * end + 1):

            @pl.when(place > 1 - y)
            def _():
                combine(place, some)

        @pl.when(borrows)
        def _():
            for h in some:
                lent = m.lent_back[:, h * HEAD : (h + 1) * HEAD].astype(jnp.float32)
                m.part[1 - y, h] += lent * jnp.exp2(m.carry[1 - y, h])

        m.att[t, j] = jnp.concatenate([m.part[1 - y, h] for h in some], axis=1).astype(jnp.bfloat16)
        start([head_copy(j, shift) for shift in range(1, tp)])

    def attention_rows(slot, j):
        return m.win[slot, 0, HEAD * batches[j][0] : HEAD * (batches[j][-1] + 1), :]

    mixed = mm(m.rec[t], m.win[t, 1])
    for j in range(len(batches)):
        mixed = mixed + mm(m.att[t, j], attention_rows(t, j))
    for shift in range(1, tp):
        slot = lax.rem(t + tp - shift, tp)
        outer_share(shift).wait_recv()
        head_copy(len(batches), shift).wait_recv()
        mixed = mixed + mm(m.rec[slot], m.win[slot, 1])
    m.sum[...] = mixed
    for shift in range(1, tp):
        slot = lax.rem(t + tp - shift, tp)
        for j in range(len(batches)):
            head_copy(j, shift).wait_recv()
            mixed = mm(m.att[slot, j], attention_rows(slot, j))
            if shift == tp - 1 and j == len(batches) - 1:
                m.out[...] = (m.sum[...] + mixed).astype(jnp.bfloat16)
            else:
                m.sum[...] += mixed

    for shift in range(1, tp):
        remote(m.tok.at[t], m.tok.at[t], m.tok_send.at[shift - 1], m.tok_recv.at[0, 0], tp=partner(shift)).wait_send()
    several = pl.ds(0, GROUP - 1)
    remote(m.s_own.at[several], m.s_own.at[several], m.s_send, m.s_recv.at[0], sp=sibling).wait_send()
    remote(m.i_own.at[several], m.i_own.at[several], m.i_send, m.i_recv.at[0], sp=sibling).wait_send()
    sent([head_copy(i, shift) for i in range(len(batches) + 1) for shift in range(1, tp)])
    sent([outer_share(shift) for shift in range(1, tp)] + [outer_copy(shift, outer[0], 0) for shift in range(1, tp)])

    @pl.loop(z + 1, planes)
    def _(plane):
        p_copy(plane).wait_send()

    @pl.loop(borrows.astype(jnp.int32), z + 1)
    def _(zs):
        relay(zs, y, None, lambda one: one.wait_send())

        @pl.when((zs < z) | (y == 1) | lends)
        def _():
            relay(zs, 1 - y, None, lambda one: one.wait_send())

    @pl.when(borrows)
    def _():
        query_copy().wait_send()

    @pl.when(lends)
    def _():
        lent_copy().wait_send()


def shards(sp, tp, *arrays):
    (tokens, gain, wq, wk, wv, bias, wr, wf, wi, wg, low, spike, norm, attention_out, recurrence_out) = arrays
    rows, features = tokens.shape
    width, wide, narrow = wq.shape[1], wr.shape[1], wi.shape[1]
    heads = width // HEAD
    columns = attention_out.shape[1] // tp
    chunks = CHUNKS
    planes = sp // GROUP
    batch = min(LANES, width)
    bf16, f32, dma = jnp.bfloat16, jnp.float32, pltpu.SemaphoreType.DMA
    inputs = dict(
        tokens=tokens,
        gain=gain.reshape(1, -1),
        hbm_k=wk,
        hbm_v=wv,
        hbm_q=wq,
        hbm_r=wr,
        hbm_f=wf,
        hbm_i=wi,
        hbm_g=wg,
        bias=bias,
        low=low,
        spike_t=spike.T,
        norm=norm.reshape(1, -1),
        hbm_attention_out=attention_out,
        hbm_recurrence_out=recurrence_out,
    )
    in_hbm = [name == "tokens" or name.startswith("hbm") for name in inputs]
    specs = [SMEM if name == "bias" else ANY if hbm else VMEM for name, hbm in zip(inputs, in_hbm)]
    scratch = dict(tok=pltpu.VMEM((tp, rows, features), bf16))
    sizes = dict(k=width, v=width, q=width, r=wide, f=wide, i=narrow, g=narrow)
    for name, size in sizes.items():
        scratch["w" + name] = pltpu.VMEM((features * tp, size), bf16)
        scratch["a" + name] = pltpu.VMEM((rows, size), f32)
        if name in "qrfig":
            scratch["p" + name] = pltpu.VMEM((rows, size), bf16)
    scratch.update(
        own_scaled=pltpu.VMEM((rows, features), bf16),
        far_scaled=pltpu.VMEM((rows, features), bf16),
        square=pltpu.VMEM((rows, LANES), f32),
        kv=pltpu.VMEM((sp, rows, 2 * width), bf16),
        qh=pltpu.VMEM((heads, rows, HEAD), bf16),
        part=pltpu.VMEM((max(4, 2 * planes), heads, rows, HEAD), f32),
        carry=pltpu.VMEM((max(4, 2 * planes), heads, rows, HEAD), f32),
        local_out=pltpu.VMEM((rows, narrow), f32),
        half_state=pltpu.VMEM((REC_VAL, wide), f32),
        half_total=pltpu.VMEM((1, wide), f32),
        qdec=pltpu.VMEM((rows, wide), bf16),
        s_own=pltpu.VMEM((GROUP, REC_VAL // GROUP + TAIL, wide), bf16),
        s_mates=pltpu.VMEM((GROUP, REC_VAL // GROUP + TAIL, wide), bf16),
        p_own=pltpu.VMEM((REC_VAL // GROUP + TAIL, wide), bf16),
        p_planes=pltpu.VMEM((planes, REC_VAL // GROUP + TAIL, wide), bf16),
        i_own=pltpu.VMEM((GROUP, REC_VAL // GROUP, wide), bf16),
        i_mates=pltpu.VMEM((GROUP, REC_VAL // GROUP, wide), bf16),
        win=pltpu.VMEM((tp, 2, width, columns), bf16),
        far_q=pltpu.VMEM((rows, width), bf16),
        lent=pltpu.VMEM((rows, width), bf16),
        lent_back=pltpu.VMEM((rows, width), bf16),
        att=pltpu.VMEM((tp, width // batch, rows, batch), bf16),
        sum=pltpu.VMEM((rows, columns), f32),
        rec=pltpu.VMEM((tp, rows, narrow), bf16),
        load_sem=dma((10,)),
        tok_send=dma((max(tp - 1, 1),)),
        tok_recv=dma((max(tp - 1, 1), chunks)),
        kv_send=dma((3, sp // 2)),
        kv_recv=dma((sp // 2, chunks)),
        sib_recv=dma((sp // 2,)),
        lend_send=dma((2,)),
        lend_recv=dma((2,)),
        s_send=dma,
        s_recv=dma((GROUP - 1,)),
        p_send=dma((planes,)),
        p_recv=dma((planes,)),
        i_send=dma,
        i_recv=dma((GROUP - 1,)),
        outer_send=dma((max(tp - 1, 1), 2)),
        outer_recv=dma((max(tp - 1, 1), 2)),
        head_send=dma((width // batch + 1, max(tp - 1, 1))),
        head_recv=dma((width // batch + 1, max(tp - 1, 1))),
    )
    return pl.pallas_call(
        functools.partial(layer_kernel, sp, tp, list(inputs) + ["out"] + list(scratch)),
        out_shape=jax.ShapeDtypeStruct((rows, columns), bf16),
        in_specs=specs,
        out_specs=VMEM,
        scratch_shapes=list(scratch.values()),
        compiler_params=pltpu.CompilerParams(
            collective_id=0, has_side_effects=True, vmem_limit_bytes=60 * 1024 * 1024
        ),
        name="layer",
    )(*inputs.values())


def solution(mesh):
    placed = (
        P("sp", "tp"),
        P(),
        P(None, "tp"),
        P(None, "tp"),
        P(None, "tp"),
        P("tp"),
        P(None, "tp"),
        P(None, "tp"),
        P(None, "tp"),
        P(None, "tp"),
        P("tp", None),
        P("sp", "tp"),
        P(),
        P("tp", None),
        P("tp", None),
    )
    return jax.shard_map(
        functools.partial(shards, mesh.shape["sp"], mesh.shape["tp"]),
        mesh=mesh,
        in_specs=placed,
        out_specs=P("sp", "tp"),
        check_vma=False,
    )
```

```python
import functools
import math
import types

import jax
import jax.numpy as jnp
from jax import lax
from jax.experimental import pallas as pl
from jax.experimental.pallas import tpu as pltpu
from jax.sharding import PartitionSpec as P

HEAD = 64
REC_KEY = 128
REC_VAL = 64
LANES = 128
GROUP = 4
TAIL = 16
CHUNKS = 4
LOG2E = math.log2(math.e)
epsilon = 1e-06
VMEM = pl.BlockSpec(memory_space=pltpu.VMEM)
SMEM = pl.BlockSpec(memory_space=pltpu.SMEM)
ANY = pl.BlockSpec(memory_space=pl.ANY)
NT = (((1,), (1,)), ((), ()))
TN = (((0,), (0,)), ((), ()))


def mm(a, b, dims=(((1,), (0,)), ((), ()))):
    return lax.dot_general(a, b, dims, preferred_element_type=jnp.float32)


def split(x):
    hi = x.astype(jnp.bfloat16)
    return hi, (x - hi.astype(jnp.float32)).astype(jnp.bfloat16)


def iota(shape, dim):
    return lax.broadcasted_iota(jnp.int32, shape, dim)


def start(copies):
    for one in copies:
        one.start()


def sent(copies):
    for one in copies:
        one.wait_send()


def remote(src, dst, send_sem, recv_sem, **target):
    return pltpu.make_async_remote_copy(
        src_ref=src,
        dst_ref=dst,
        send_sem=send_sem,
        recv_sem=recv_sem,
        device_id=target,
        device_id_type=pl.DeviceIdType.MESH,
    )


def tail_of(total):
    hi, lo = split(total)
    lo, rest = split(total - hi.astype(jnp.float32))
    which = iota((TAIL, total.shape[1]), 0)
    tail = jnp.where(which == 0, hi.astype(jnp.float32), jnp.where(which == 1, lo.astype(jnp.float32), 0.0))
    return jnp.where(which == 2, rest.astype(jnp.float32), tail).astype(jnp.bfloat16)


def layer_kernel(sp, tp, names, *refs):
    m = types.SimpleNamespace(**dict(zip(names, refs)))
    rows, features = m.tok.shape[1:]
    width, wide, narrow = m.wk.shape[1], m.wr.shape[1], m.wi.shape[1]
    heads, rec_heads = width // HEAD, narrow // REC_VAL
    chunks, chunk = CHUNKS, rows // CHUNKS
    planes = sp // GROUP
    lend = planes > 2
    columns = m.out.shape[1]
    span = REC_VAL // GROUP
    together = m.att.shape[3] // HEAD
    batches = [range(h, h + together) for h in range(0, heads, together)]
    me, t = lax.axis_index("sp"), lax.axis_index("tp")
    c, y, z = lax.rem(me, 2), lax.rem(me // 2, 2), me // GROUP
    g = lax.rem(me, GROUP)
    sibling, across = me + 1 - 2 * c, z * GROUP + (1 - y) * 2 + c
    ahead = lax.rem(z + 1, planes) * GROUP + g
    bottom, top = g, (planes - 1) * GROUP + g
    lends, borrows = lend & (z == 0), lend & (z == planes - 1)

    def mate(off):
        return z * GROUP + lax.rem(g + off, GROUP)

    def partner(shift):
        return lax.rem(t + shift, tp)

    load_tokens = pltpu.make_async_copy(m.tokens, m.tok.at[t], m.load_sem.at[0])
    load_tokens.start()
    order = "krfivqg"
    loads = [
        pltpu.make_async_copy(getattr(m, "hbm_" + name), getattr(m, "w" + name), m.load_sem.at[1 + i])
        for i, name in enumerate(order)
    ]
    start(loads)
    own_columns = pl.ds(pl.multiple_of(t * columns, columns), columns)
    outer = (m.hbm_attention_out, m.hbm_recurrence_out)
    load_outer = [
        pltpu.make_async_copy(array.at[:, own_columns], m.win.at[t, i], m.load_sem.at[8 + i])
        for i, array in enumerate(outer)
    ]
    start(load_outer)

    barrier = pltpu.get_barrier_semaphore()
    for off in range(1, GROUP):
        pl.semaphore_signal(barrier, inc=1, device_id={"sp": mate(off)}, device_id_type=pl.DeviceIdType.MESH)
    for off in range(1, planes):
        peer = lax.rem(z + off, planes) * GROUP + g
        pl.semaphore_signal(barrier, inc=1, device_id={"sp": peer}, device_id_type=pl.DeviceIdType.MESH)
    for shift in range(1, tp):
        pl.semaphore_signal(barrier, inc=1, device_id={"tp": partner(shift)}, device_id_type=pl.DeviceIdType.MESH)
    pl.semaphore_wait(barrier, GROUP + planes + tp - 3)
    load_tokens.wait()

    def token_copy(shift, r, slot):
        part = m.tok.at[slot, pl.ds(r * chunk, chunk)]
        return remote(part, part, m.tok_send.at[shift - 1], m.tok_recv.at[shift - 1, r], tp=partner(shift))

    token_sends = [token_copy(shift, r, t) for shift in range(1, tp) for r in range(chunks)]
    start(token_sends)

    def scale(slot, part):
        value = m.tok[slot, part, :].astype(jnp.float32)
        gains = m.gain[:, pl.ds(pl.multiple_of(slot * features, features), features)]
        return (value * gains).astype(jnp.bfloat16), jnp.sum(value * value, axis=1, keepdims=True)

    def weight_rows(name, slot, cut):
        return getattr(m, "w" + name)[pl.ds(pl.multiple_of(slot * features, features), features), cut]

    def tiles(name):
        size = getattr(m, "w" + name).shape[1]
        step = min(256, size)
        return [slice(i, i + step) for i in range(0, size, step)]

    scaled, squares = scale(t, slice(0, rows))
    m.own_scaled[...] = scaled
    m.square[...] = jnp.broadcast_to(squares, m.square.shape)
    for load, name in zip(loads, order):
        load.wait()
        for cut in tiles(name):
            getattr(m, "a" + name)[:, cut] = mm(m.own_scaled[...], weight_rows(name, t, cut))

    def kv_copy(number, r, way, target):
        piece = m.kv.at[number, pl.ds(r * chunk, chunk)]
        kind = number // 2
        if way == 2:
            return remote(piece, piece, m.kv_send.at[2, kind], m.sib_recv.at[kind], sp=target)
        return remote(piece, piece, m.kv_send.at[way, kind], m.kv_recv.at[kind, r], sp=target)

    def kv_whole(number, way):
        piece, kind = m.kv.at[number], number // 2
        return remote(piece, piece, m.kv_send.at[way, kind], m.sib_recv.at[kind], sp=sibling)

    def relay(zs, ys, r, act):
        copy = kv_copy if r is not None else lambda number, r, way, target: kv_whole(number, way)
        number = zs * GROUP + ys * 2 + c
        column, here = ys == y, zs == z
        last = jnp.where(zs == 0, planes - 1 - lend, planes - 1)

        @pl.when(column & (z < last))
        def _():
            act(copy(number, r, 0, ahead))

        @pl.when(column & (~here | (y == 0) | lends))
        def _():
            act(copy(number, r, 1, across))

        @pl.when(~here | (column & (c == 0)) | (~column & (y == 1)) | lends)
        def _():
            act(copy(number, r, 2, sibling))

    def event(cond, zs, ys, r):
        @pl.when(cond & ~(borrows & (zs == 0)))
        def _():
            kv_copy(zs * GROUP + ys * 2 + c, r, 0, ahead).wait_recv()
            relay(zs, ys, r, lambda one: one.start())

    def facing(w):
        return (w <= z + 1) & ((w > 1) | (y == 1) | lends)

    def wave_events(w, r):
        event(w <= z, z - w, y, r)
        event(facing(w), z - w + 1, 1 - y, r)

    def from_sibling(zs, ys):
        kv_whole(zs * GROUP + ys * 2 + 1 - c, 2).wait_recv()

    part_rows = rows // 2
    r_iota, c_iota = iota((part_rows, part_rows), 0), iota((part_rows, part_rows), 1)
    causal = r_iota >= c_iota
    lower = causal.astype(jnp.bfloat16)
    upper = (r_iota <= c_iota).astype(jnp.bfloat16)

    def project(name, part):
        inverse = lax.rsqrt(m.square[part, 0:1] * (1.0 / (features * tp)) + epsilon)
        for cut in tiles(name):
            whole = getattr(m, "a" + name)[part, cut] + mm(
                m.far_scaled[part], weight_rows(name, lax.rem(t + 1, tp), cut)
            )
            getattr(m, "p" + name)[part, cut] = (whole * inverse).astype(jnp.bfloat16)

    def recur(which):
        part = slice(which * part_rows, (which + 1) * part_rows)
        spikes = m.spike_t[:, part]
        if rec_heads == 1:
            spikes = jnp.broadcast_to(spikes, (8, part_rows))
        hi, lo = split(spikes)
        spike_col = mm(lower, hi, NT) + mm(lower, lo, NT)
        spike_row = mm(hi, upper) + mm(lo, upper)
        for h in range(rec_heads):
            ks = slice(h * REC_KEY, (h + 1) * REC_KEY)
            vs = slice(h * REC_VAL, (h + 1) * REC_VAL)
            q = m.pr[part, ks].astype(jnp.float32)
            lifted = q * jax.nn.sigmoid(q)
            intake = (1.0 - m.low[h : h + 1, :]) * jax.nn.sigmoid(-m.pf[part, ks].astype(jnp.float32))
            hi, lo = split(jnp.log1p(-intake))
            run = mm(lower, hi) + mm(lower, lo)
            s_col = spike_col[:, h : h + 1]
            s_row = spike_row[h : h + 1, :]
            q_up = lifted * jnp.exp(run)
            k_down = (intake * jnp.exp(-run)).astype(jnp.bfloat16)
            decay = jnp.exp(jnp.where(causal, s_col - s_row, 0.0))
            inner = jnp.where(causal, mm(q_up.astype(jnp.bfloat16), k_down, NT) * decay, 0.0)
            v = m.pi[part, vs]
            output = mm(inner.astype(jnp.bfloat16), v)
            decayed = q_up * jnp.exp(s_col)
            total = run[part_rows - 1 : part_rows, :] + s_col[part_rows - 1 : part_rows, :]
            k_end = (intake * jnp.exp(total - (run + s_col))).astype(jnp.bfloat16)
            state = mm(v, k_end, TN)
            if which == 0:
                m.local_out[part, vs] = output
                m.qdec[part, ks] = decayed.astype(jnp.bfloat16)
                m.half_state[:, ks] = state
                m.half_total[:, ks] = total
                continue
            earlier = m.half_state[:, ks]
            m.local_out[part, vs] = output + mm(decayed.astype(jnp.bfloat16), earlier.astype(jnp.bfloat16), NT)
            m.qdec[part, ks] = (decayed * jnp.exp(m.half_total[:, ks])).astype(jnp.bfloat16)
            state = (earlier * jnp.exp(total) + state).astype(jnp.bfloat16)
            tail = tail_of(total + m.half_total[:, ks])
            for i in range(GROUP):
                m.s_own[i, 0:span, ks] = state[i * span : (i + 1) * span]
                m.s_own[i, span:, ks] = tail

    first_rows, last_rows = slice(0, part_rows), slice(part_rows, rows)

    for shift in range(1, tp):
        slot = lax.rem(t + tp - shift, tp)
        for r in range(chunks):
            part = slice(r * chunk, (r + 1) * chunk)
            token_copy(shift, r, slot).wait_recv()
            scaled, squares = scale(slot, part)
            m.far_scaled[part] = scaled
            m.square[part] += jnp.broadcast_to(squares, (chunk, LANES))
            if shift == tp - 1:
                inverse = lax.rsqrt(m.square[part, 0:1] * (1.0 / (features * tp)) + epsilon)
                for i, name in enumerate("kv"):
                    whole = getattr(m, "a" + name)[part, :] + mm(
                        m.far_scaled[part], weight_rows(name, slot, slice(0, width))
                    )
                    m.kv[me, part, i * width : (i + 1) * width] = (whole * inverse).astype(jnp.bfloat16)
                relay(z, y, r, lambda one: one.start())
                if 0 < r < chunks - 1:
                    wave_events(1, r - 1)
                if r == chunks // 2 - 1:
                    for name in "qrfi":
                        project(name, first_rows)
                    recur(0)
        if shift < tp - 1:
            for name in order:
                for cut in tiles(name):
                    getattr(m, "a" + name)[:, cut] += mm(m.far_scaled[...], weight_rows(name, slot, cut))
    slot = lax.rem(t + 1, tp)
    def outer_copy(shift, array, other):
        from_columns = array.at[:, pl.ds(pl.multiple_of(partner(shift) * columns, columns), columns)]
        return remote(
            from_columns, m.win.at[t, other], m.outer_send.at[shift - 1, 0], m.outer_recv.at[shift - 1, 0], tp=partner(shift)
        )

    for which, array in enumerate(outer):

        @pl.when(c == which)
        def _():
            start([outer_copy(shift, array, which) for shift in range(1, tp)])

    def outer_share(shift):
        piece = m.win.at[lax.rem(t + tp - shift, tp), c]
        return remote(piece, piece, m.outer_send.at[shift - 1, 1], m.outer_recv.at[shift - 1, 1], sp=sibling)

    def query_copy():
        return remote(m.pq, m.far_q, m.lend_send.at[0], m.lend_recv.at[0], sp=bottom)

    def lent_copy():
        return remote(m.lent, m.lent_back, m.lend_send.at[1], m.lend_recv.at[1], sp=top)

    project("q", last_rows)

    @pl.when(borrows)
    def _():
        query_copy().start()

    for name in "rfi":
        project(name, last_rows)
    wave_events(1, chunks - 2)
    wave_events(2, 0)
    recur(1)

    def s_copy(off):
        return remote(
            m.s_own.at[lax.rem(g + off, GROUP)], m.s_mates.at[g], m.s_send, m.s_recv.at[off - 1], sp=mate(off)
        )

    def p_copy(plane):
        return remote(m.p_own, m.p_planes.at[z], m.p_send.at[plane], m.p_recv.at[z], sp=plane * GROUP + g)

    def p_arrival(plane):
        return remote(m.p_own, m.p_planes.at[plane], m.p_send.at[plane], m.p_recv.at[plane], sp=bottom)

    def i_copy(off):
        return remote(
            m.i_own.at[lax.rem(g + off, GROUP)], m.i_mates.at[g], m.i_send, m.i_recv.at[off - 1], sp=mate(off)
        )

    start([s_copy(off) for off in range(1, GROUP)])
    project("g", slice(0, rows))
    wave_events(1, chunks - 1)
    wave_events(2, 1)
    m.s_mates[g] = m.s_own[g]

    def take_queries(queries):
        for h in range(heads):
            m.qh[h] = queries[:, h * HEAD : (h + 1) * HEAD]

    take_queries(m.pq)

    def parts(packed):
        return packed[0:span].astype(jnp.float32), jnp.sum(packed[span:].astype(jnp.float32), axis=0, keepdims=True)

    def append(state, packed):
        added, total = parts(packed)
        return state * jnp.exp(total) + added

    r_iota, c_iota = iota((rows, rows), 0), iota((rows, rows), 1)
    sums = jnp.where(r_iota > c_iota, -1.0, 0.0).astype(jnp.bfloat16)
    before = c_iota < r_iota

    def attend(numbers, place, first=False, after=False, some=range(heads)):
        scores, stays = [], []
        for number in numbers:
            for h in some:
                hs = slice(h * HEAD, (h + 1) * HEAD)
                s = mm(m.qh[h], m.kv[number, :, hs], NT) * (HEAD**-0.5 * LOG2E) + m.bias[h] * LOG2E
                soft = jnp.maximum(s, jnp.log2(1.0 + jnp.exp2(jnp.minimum(s, 100.0))))
                scores.append(s - soft)
                stays.append(jnp.where(before, soft, 0.0) if first else soft)
        done = {}
        for i, (score, stay) in enumerate(zip(scores, stays)):
            number, h = numbers[i // len(some)], some[i % len(some)]
            vs = slice(width + h * HEAD, width + (h + 1) * HEAD)
            later = mm(stay.astype(jnp.bfloat16), sums)
            w = jnp.exp2(score + later)
            if first:
                w = jnp.where(before, w, 0.0)
            o = mm(w.astype(jnp.bfloat16), m.kv[number, :, vs])
            every = jnp.broadcast_to((later - stay)[:, 0:1], (rows, HEAD))
            if after:
                done[h] = m.part[place, h], m.carry[place, h]
            if h in done:
                o, every = done[h][0] + o * jnp.exp2(done[h][1]), done[h][1] + every
            done[h] = o, every
            if number is numbers[-1]:
                m.part[place, h], m.carry[place, h] = done[h]

    attend([me], 1 - y, first=True)

    @pl.when(c == 1)
    def _():
        from_sibling(z, y)
        attend([me - 1], 1 - y, after=True)

    def combine(place, some=range(heads)):
        for h in some:
            m.part[1 - y, h] += m.part[place, h] * jnp.exp2(m.carry[1 - y, h])
            m.carry[1 - y, h] += m.carry[place, h]

    def combine_wave(w):
        for place in (2 * w - 2, 2 * w - 1):

            @pl.when(place > 1 - y)
            def _():
                combine(place)

    def gather_states():
        for off in range(1, GROUP):
            s_copy(off).wait_recv()
        state, total = parts(m.s_mates[0])
        for i in range(1, GROUP):
            state = append(state, m.s_mates[i])
            total = total + parts(m.s_mates[i])[1]
        m.p_own[0:span] = state.astype(jnp.bfloat16)
        m.p_own[span:] = tail_of(total)

        @pl.loop(z + 1, planes)
        def _(plane):
            p_copy(plane).start()

    def enter_states():
        @pl.loop(0, z)
        def _(plane):
            p_arrival(plane).wait_recv()

        state = lax.fori_loop(
            0, z, lambda plane, so_far: append(so_far, m.p_planes[plane]), jnp.zeros((span, wide), jnp.float32)
        )
        for i in range(GROUP):
            m.i_own[i] = state.astype(jnp.bfloat16)
            state = append(state, m.s_mates[i])
        start([i_copy(off) for off in range(1, GROUP)])
        m.i_mates[g] = m.i_own[g]

    def head_copy(i, shift):
        piece = m.rec.at[t] if i == len(batches) else m.att.at[t, i]
        return remote(piece, piece, m.head_send.at[i, shift - 1], m.head_recv.at[i, shift - 1], tp=partner(shift))

    def finish_states():
        for off in range(1, GROUP):
            i_copy(off).wait_recv()
        for h in range(rec_heads):
            ks = slice(h * REC_KEY, (h + 1) * REC_KEY)
            vs = slice(h * REC_VAL, (h + 1) * REC_VAL)
            entering = jnp.concatenate([m.i_mates[i, :, ks] for i in range(GROUP)], axis=0)
            raw = m.local_out[:, vs] + mm(m.qdec[:, ks], entering, NT)
            gate = m.pg[:, vs].astype(jnp.float32)
            mean = jnp.sum(raw * raw, axis=1, keepdims=True) * (1.0 / REC_VAL)
            done = raw * lax.rsqrt(mean + epsilon) * m.norm[...] * (gate * jax.nn.sigmoid(gate))
            m.rec[t, :, vs] = done.astype(jnp.bfloat16)
        start([head_copy(len(batches), shift) for shift in range(1, tp)])

    waves = z + 1 - borrows.astype(jnp.int32)

    @pl.loop(1, waves + 1)
    def _(w):
        @pl.when(w > 1)
        def _():
            combine_wave(w - 1)
            wave_events(w, chunks - 1)

        @pl.when(w == 3)
        def _():
            finish_states()

        @pl.loop(0, 2)
        def _(i):
            zs, ys = z - w + 1 - i, jnp.where(i == 0, 1 - y, y)

            @pl.when((i == 1) & (zs >= 0) & ~(borrows & (zs == 0)) | (i == 0) & ((w > 1) | (y == 1)) & (w < waves))
            def _():
                from_sibling(zs, ys)
                attend([zs * GROUP + ys * 2 + 1, zs * GROUP + ys * 2], 2 * (z - zs) + 1 - ys)

            @pl.when((w == 1) & (i == 0))
            def _():
                for r in range(2, chunks - 1):
                    wave_events(2, r)

            @pl.when((w > 1) & (i == 0))
            def _():
                for r in range(chunks - 1):
                    wave_events(w + 1, r)

            @pl.when((w == 2) & (i == 0))
            def _():
                enter_states()

        @pl.when(w == 1)
        def _():
            gather_states()

    @pl.when(z == 0)
    def _():
        enter_states()

    if lend:

        @pl.when(z == 0)
        def _():
            query_copy().wait_recv()
            take_queries(m.far_q)

            @pl.when(c == 0)
            def _():
                from_sibling(0, y)

            from_sibling(0, 1 - y)

            @pl.loop(0, 2)
            def _(i):
                attend([3 - 2 * i, 2 - 2 * i], 2 + i)

            for h in range(heads):
                whole = m.part[2, h] + m.part[3, h] * jnp.exp2(m.carry[2, h])
                m.lent[:, h * HEAD : (h + 1) * HEAD] = whole.astype(jnp.bfloat16)
            lent_copy().start()
            take_queries(m.pq)

    @pl.when(z < 2)
    def _():
        finish_states()

    for shift in range(1, tp):
        outer_copy(shift, outer[0], 0).wait_recv()
        outer_share(shift).start()
    for one in load_outer:
        one.wait()

    end, last = waves - 1, z - waves + 1
    facing_end = (waves > 1) | (y == 1)

    @pl.when(facing_end & ~lends)
    def _():
        from_sibling(last, 1 - y)

    @pl.when(borrows)
    def _():
        lent_copy().wait_recv()

    for j, some in enumerate(batches):

        @pl.when(facing_end)
        def _():
            attend([last * GROUP + (1 - y) * 2 + 1, last * GROUP + (1 - y) * 2], 2 * end + y, some=some)

        for place in (2 * end, 2 * end + 1):

            @pl.when(place > 1 - y)
            def _():
                combine(place, some)

        @pl.when(borrows)
        def _():
            for h in some:
                lent = m.lent_back[:, h * HEAD : (h + 1) * HEAD].astype(jnp.float32)
                m.part[1 - y, h] += lent * jnp.exp2(m.carry[1 - y, h])

        m.att[t, j] = jnp.concatenate([m.part[1 - y, h] for h in some], axis=1).astype(jnp.bfloat16)
        start([head_copy(j, shift) for shift in range(1, tp)])

    def attention_rows(slot, j):
        return m.win[slot, 0, HEAD * batches[j][0] : HEAD * (batches[j][-1] + 1), :]

    mixed = mm(m.rec[t], m.win[t, 1])
    for j in range(len(batches)):
        mixed = mixed + mm(m.att[t, j], attention_rows(t, j))
    for shift in range(1, tp):
        slot = lax.rem(t + tp - shift, tp)
        outer_share(shift).wait_recv()
        head_copy(len(batches), shift).wait_recv()
        mixed = mixed + mm(m.rec[slot], m.win[slot, 1])
    m.sum[...] = mixed
    for shift in range(1, tp):
        slot = lax.rem(t + tp - shift, tp)
        for j in range(len(batches)):
            head_copy(j, shift).wait_recv()
            mixed = mm(m.att[slot, j], attention_rows(slot, j))
            if shift == tp - 1 and j == len(batches) - 1:
                m.out[...] = (m.sum[...] + mixed).astype(jnp.bfloat16)
            else:
                m.sum[...] += mixed

    for shift in range(1, tp):
        remote(m.tok.at[t], m.tok.at[t], m.tok_send.at[shift - 1], m.tok_recv.at[0, 0], tp=partner(shift)).wait_send()
    several = pl.ds(0, GROUP - 1)
    remote(m.s_own.at[several], m.s_own.at[several], m.s_send, m.s_recv.at[0], sp=sibling).wait_send()
    remote(m.i_own.at[several], m.i_own.at[several], m.i_send, m.i_recv.at[0], sp=sibling).wait_send()
    sent([head_copy(i, shift) for i in range(len(batches) + 1) for shift in range(1, tp)])
    sent([outer_share(shift) for shift in range(1, tp)] + [outer_copy(shift, outer[0], 0) for shift in range(1, tp)])

    @pl.loop(z + 1, planes)
    def _(plane):
        p_copy(plane).wait_send()

    @pl.loop(borrows.astype(jnp.int32), z + 1)
    def _(zs):
        relay(zs, y, None, lambda one: one.wait_send())

        @pl.when((zs < z) | (y == 1) | lends)
        def _():
            relay(zs, 1 - y, None, lambda one: one.wait_send())

    @pl.when(borrows)
    def _():
        query_copy().wait_send()

    @pl.when(lends)
    def _():
        lent_copy().wait_send()


def shards(sp, tp, *arrays):
    (tokens, gain, wq, wk, wv, bias, wr, wf, wi, wg, low, spike, norm, attention_out, recurrence_out) = arrays
    rows, features = tokens.shape
    width, wide, narrow = wq.shape[1], wr.shape[1], wi.shape[1]
    heads = width // HEAD
    columns = attention_out.shape[1] // tp
    chunks = CHUNKS
    planes = sp // GROUP
    batch = min(LANES, width)
    bf16, f32, dma = jnp.bfloat16, jnp.float32, pltpu.SemaphoreType.DMA
    inputs = dict(
        tokens=tokens,
        gain=gain.reshape(1, -1),
        hbm_k=wk,
        hbm_v=wv,
        hbm_q=wq,
        hbm_r=wr,
        hbm_f=wf,
        hbm_i=wi,
        hbm_g=wg,
        bias=bias,
        low=low,
        spike_t=spike.T,
        norm=norm.reshape(1, -1),
        hbm_attention_out=attention_out,
        hbm_recurrence_out=recurrence_out,
    )
    in_hbm = [name == "tokens" or name.startswith("hbm") for name in inputs]
    specs = [SMEM if name == "bias" else ANY if hbm else VMEM for name, hbm in zip(inputs, in_hbm)]
    scratch = dict(tok=pltpu.VMEM((tp, rows, features), bf16))
    sizes = dict(k=width, v=width, q=width, r=wide, f=wide, i=narrow, g=narrow)
    for name, size in sizes.items():
        scratch["w" + name] = pltpu.VMEM((features * tp, size), bf16)
        scratch["a" + name] = pltpu.VMEM((rows, size), f32)
        if name in "qrfig":
            scratch["p" + name] = pltpu.VMEM((rows, size), bf16)
    scratch.update(
        own_scaled=pltpu.VMEM((rows, features), bf16),
        far_scaled=pltpu.VMEM((rows, features), bf16),
        square=pltpu.VMEM((rows, LANES), f32),
        kv=pltpu.VMEM((sp, rows, 2 * width), bf16),
        qh=pltpu.VMEM((heads, rows, HEAD), bf16),
        part=pltpu.VMEM((max(4, 2 * planes), heads, rows, HEAD), f32),
        carry=pltpu.VMEM((max(4, 2 * planes), heads, rows, HEAD), f32),
        local_out=pltpu.VMEM((rows, narrow), f32),
        half_state=pltpu.VMEM((REC_VAL, wide), f32),
        half_total=pltpu.VMEM((1, wide), f32),
        qdec=pltpu.VMEM((rows, wide), bf16),
        s_own=pltpu.VMEM((GROUP, REC_VAL // GROUP + TAIL, wide), bf16),
        s_mates=pltpu.VMEM((GROUP, REC_VAL // GROUP + TAIL, wide), bf16),
        p_own=pltpu.VMEM((REC_VAL // GROUP + TAIL, wide), bf16),
        p_planes=pltpu.VMEM((planes, REC_VAL // GROUP + TAIL, wide), bf16),
        i_own=pltpu.VMEM((GROUP, REC_VAL // GROUP, wide), bf16),
        i_mates=pltpu.VMEM((GROUP, REC_VAL // GROUP, wide), bf16),
        win=pltpu.VMEM((tp, 2, width, columns), bf16),
        far_q=pltpu.VMEM((rows, width), bf16),
        lent=pltpu.VMEM((rows, width), bf16),
        lent_back=pltpu.VMEM((rows, width), bf16),
        att=pltpu.VMEM((tp, width // batch, rows, batch), bf16),
        sum=pltpu.VMEM((rows, columns), f32),
        rec=pltpu.VMEM((tp, rows, narrow), bf16),
        load_sem=dma((10,)),
        tok_send=dma((max(tp - 1, 1),)),
        tok_recv=dma((max(tp - 1, 1), chunks)),
        kv_send=dma((3, sp // 2)),
        kv_recv=dma((sp // 2, chunks)),
        sib_recv=dma((sp // 2,)),
        lend_send=dma((2,)),
        lend_recv=dma((2,)),
        s_send=dma,
        s_recv=dma((GROUP - 1,)),
        p_send=dma((planes,)),
        p_recv=dma((planes,)),
        i_send=dma,
        i_recv=dma((GROUP - 1,)),
        outer_send=dma((max(tp - 1, 1), 2)),
        outer_recv=dma((max(tp - 1, 1), 2)),
        head_send=dma((width // batch + 1, max(tp - 1, 1))),
        head_recv=dma((width // batch + 1, max(tp - 1, 1))),
    )
    return pl.pallas_call(
        functools.partial(layer_kernel, sp, tp, list(inputs) + ["out"] + list(scratch)),
        out_shape=jax.ShapeDtypeStruct((rows, columns), bf16),
        in_specs=specs,
        out_specs=VMEM,
        scratch_shapes=list(scratch.values()),
        compiler_params=pltpu.CompilerParams(
            collective_id=0, has_side_effects=True, vmem_limit_bytes=60 * 1024 * 1024
        ),
        name="layer",
    )(*inputs.values())


def solution(mesh):
    placed = (
        P("sp", "tp"),
        P(),
        P(None, "tp"),
        P(None, "tp"),
        P(None, "tp"),
        P("tp"),
        P(None, "tp"),
        P(None, "tp"),
        P(None, "tp"),
        P(None, "tp"),
        P("tp", None),
        P("sp", "tp"),
        P(),
        P("tp", None),
        P("tp", None),
    )
    return jax.shard_map(
        functools.partial(shards, mesh.shape["sp"], mesh.shape["tp"]),
        mesh=mesh,
        in_specs=placed,
        out_specs=P("sp", "tp"),
        check_vma=False,
    )
```

```python
import functools
import math
import types

import jax
import jax.numpy as jnp
from jax import lax
from jax.experimental import pallas as pl
from jax.experimental.pallas import tpu as pltpu
from jax.sharding import PartitionSpec as P

HEAD = 64
REC_KEY = 128
REC_VAL = 64
LANES = 128
GROUP = 4
TAIL = 16
CHUNKS = 4
SPIKES, LOWS = 8, 16
LOG2E = math.log2(math.e)
epsilon = 1e-06
VMEM = pl.BlockSpec(memory_space=pltpu.VMEM)
SMEM = pl.BlockSpec(memory_space=pltpu.SMEM)
ANY = pl.BlockSpec(memory_space=pl.ANY)
NT = (((1,), (1,)), ((), ()))
TN = (((0,), (0,)), ((), ()))


def mm(a, b, dims=(((1,), (0,)), ((), ()))):
    return lax.dot_general(a, b, dims, preferred_element_type=jnp.float32)


def split(x):
    hi = x.astype(jnp.bfloat16)
    return hi, (x - hi.astype(jnp.float32)).astype(jnp.bfloat16)


def iota(shape, dim):
    return lax.broadcasted_iota(jnp.int32, shape, dim)


def start(copies):
    for one in copies:
        one.start()


def sent(copies):
    for one in copies:
        one.wait_send()


def remote(src, dst, send_sem, recv_sem, **target):
    return pltpu.make_async_remote_copy(
        src_ref=src,
        dst_ref=dst,
        send_sem=send_sem,
        recv_sem=recv_sem,
        device_id=target,
        device_id_type=pl.DeviceIdType.MESH,
    )


def tail_of(total):
    hi, lo = split(total)
    lo, rest = split(total - hi.astype(jnp.float32))
    which = iota((TAIL, total.shape[1]), 0)
    tail = jnp.where(which == 0, hi.astype(jnp.float32), jnp.where(which == 1, lo.astype(jnp.float32), 0.0))
    return jnp.where(which == 2, rest.astype(jnp.float32), tail).astype(jnp.bfloat16)


def layer_kernel(sp, tp, names, *refs):
    m = types.SimpleNamespace(**dict(zip(names, refs)))
    rows, features = m.tok.shape[1:]
    width, wide, narrow = m.wk.shape[1], m.wr.shape[1], m.wi.shape[1]
    heads, rec_heads = width // HEAD, narrow // REC_VAL
    chunks, chunk = CHUNKS, rows // CHUNKS
    planes = sp // GROUP
    lend = planes > 2
    columns = m.out.shape[1]
    span = REC_VAL // GROUP
    together = m.att.shape[3] // HEAD
    batches = [range(h, h + together) for h in range(0, heads, together)]
    me, t = lax.axis_index("sp"), lax.axis_index("tp")
    c, y, z = lax.rem(me, 2), lax.rem(me // 2, 2), me // GROUP
    g = lax.rem(me, GROUP)
    sibling, across = me + 1 - 2 * c, z * GROUP + (1 - y) * 2 + c
    ahead = lax.rem(z + 1, planes) * GROUP + g
    bottom, top = g, (planes - 1) * GROUP + g
    lends, borrows = lend & (z == 0), lend & (z == planes - 1)

    def mate(off):
        return z * GROUP + lax.rem(g + off, GROUP)

    def partner(shift):
        return lax.rem(t + shift, tp)

    load_tokens = pltpu.make_async_copy(m.tokens, m.tok.at[t], m.load_sem.at[0])
    load_tokens.start()
    order = "krfivqg"
    loads = [
        pltpu.make_async_copy(getattr(m, "hbm_" + name), getattr(m, "w" + name), m.load_sem.at[1 + i])
        for i, name in enumerate(order)
    ]
    start(loads)
    own_columns = pl.ds(pl.multiple_of(t * columns, columns), columns)
    outer = (m.hbm_attention_out, m.hbm_recurrence_out)
    load_outer = [
        pltpu.make_async_copy(array.at[:, own_columns], m.win.at[t, i], m.load_sem.at[8 + i])
        for i, array in enumerate(outer)
    ]
    start(load_outer)

    barrier = pltpu.get_barrier_semaphore()
    for off in range(1, GROUP):
        pl.semaphore_signal(barrier, inc=1, device_id={"sp": mate(off)}, device_id_type=pl.DeviceIdType.MESH)
    for off in range(1, planes):
        peer = lax.rem(z + off, planes) * GROUP + g
        pl.semaphore_signal(barrier, inc=1, device_id={"sp": peer}, device_id_type=pl.DeviceIdType.MESH)
    for shift in range(1, tp):
        pl.semaphore_signal(barrier, inc=1, device_id={"tp": partner(shift)}, device_id_type=pl.DeviceIdType.MESH)
    pl.semaphore_wait(barrier, GROUP + planes + tp - 3)
    load_tokens.wait()

    def token_copy(shift, r, slot):
        part = m.tok.at[slot, pl.ds(r * chunk, chunk)]
        return remote(part, part, m.tok_send.at[shift - 1], m.tok_recv.at[shift - 1, r], tp=partner(shift))

    token_sends = [token_copy(shift, r, t) for shift in range(1, tp) for r in range(chunks)]
    start(token_sends)

    def scale(slot, part):
        value = m.tok[slot, part, :].astype(jnp.float32)
        gains = m.small[0:1, pl.ds(pl.multiple_of(slot * features, features), features)]
        return (value * gains).astype(jnp.bfloat16), jnp.sum(value * value, axis=1, keepdims=True)

    def weight_rows(name, slot, cut):
        return getattr(m, "w" + name)[pl.ds(pl.multiple_of(slot * features, features), features), cut]

    def tiles(name):
        size = getattr(m, "w" + name).shape[1]
        step = min(256, size)
        return [slice(i, i + step) for i in range(0, size, step)]

    scaled, squares = scale(t, slice(0, rows))
    m.own_scaled[...] = scaled
    m.square[...] = jnp.broadcast_to(squares, m.square.shape)
    for load, name in zip(loads, order):
        load.wait()
        for cut in tiles(name):
            getattr(m, "a" + name)[:, cut] = mm(m.own_scaled[...], weight_rows(name, t, cut))

    def kv_copy(number, r, way, target):
        piece = m.kv.at[number, pl.ds(r * chunk, chunk)]
        kind = number // 2
        if way == 2:
            return remote(piece, piece, m.kv_send.at[2, kind], m.sib_recv.at[kind], sp=target)
        return remote(piece, piece, m.kv_send.at[way, kind], m.kv_recv.at[kind, r], sp=target)

    def kv_whole(number, way):
        piece, kind = m.kv.at[number], number // 2
        return remote(piece, piece, m.kv_send.at[way, kind], m.sib_recv.at[kind], sp=sibling)

    def relay(zs, ys, r, act):
        copy = kv_copy if r is not None else lambda number, r, way, target: kv_whole(number, way)
        number = zs * GROUP + ys * 2 + c
        column, here = ys == y, zs == z
        last = jnp.where(zs == 0, planes - 1 - lend, planes - 1)

        @pl.when(column & (z < last))
        def _():
            act(copy(number, r, 0, ahead))

        @pl.when(column & (~here | (y == 0) | lends))
        def _():
            act(copy(number, r, 1, across))

        @pl.when(~here | (column & (c == 0)) | (~column & (y == 1)) | lends)
        def _():
            act(copy(number, r, 2, sibling))

    def event(cond, zs, ys, r):
        @pl.when(cond & ~(borrows & (zs == 0)))
        def _():
            kv_copy(zs * GROUP + ys * 2 + c, r, 0, ahead).wait_recv()
            relay(zs, ys, r, lambda one: one.start())

    def facing(w):
        return (w <= z + 1) & ((w > 1) | (y == 1) | lends)

    def wave_events(w, r):
        event(w <= z, z - w, y, r)
        event(facing(w), z - w + 1, 1 - y, r)

    def from_sibling(zs, ys):
        kv_whole(zs * GROUP + ys * 2 + 1 - c, 2).wait_recv()

    part_rows = rows // 2
    r_iota, c_iota = iota((part_rows, part_rows), 0), iota((part_rows, part_rows), 1)
    causal = r_iota >= c_iota
    lower = causal.astype(jnp.bfloat16)
    upper = (r_iota <= c_iota).astype(jnp.bfloat16)

    def project(name, part):
        inverse = lax.rsqrt(m.square[part, 0:1] * (1.0 / (features * tp)) + epsilon)
        for cut in tiles(name):
            whole = getattr(m, "a" + name)[part, cut] + mm(
                m.far_scaled[part], weight_rows(name, lax.rem(t + 1, tp), cut)
            )
            getattr(m, "p" + name)[part, cut] = (whole * inverse).astype(jnp.bfloat16)

    def recur(which):
        part = slice(which * part_rows, (which + 1) * part_rows)
        spikes = m.small[SPIKES : SPIKES + rec_heads, part]
        if rec_heads == 1:
            spikes = jnp.broadcast_to(spikes, (8, part_rows))
        hi, lo = split(spikes)
        spike_col = mm(lower, hi, NT) + mm(lower, lo, NT)
        spike_row = mm(hi, upper) + mm(lo, upper)
        for h in range(rec_heads):
            ks = slice(h * REC_KEY, (h + 1) * REC_KEY)
            vs = slice(h * REC_VAL, (h + 1) * REC_VAL)
            q = m.pr[part, ks].astype(jnp.float32)
            lifted = q * jax.nn.sigmoid(q)
            intake = (1.0 - m.small[LOWS + h : LOWS + h + 1, 0:REC_KEY]) * jax.nn.sigmoid(-m.pf[part, ks].astype(jnp.float32))
            hi, lo = split(jnp.log1p(-intake))
            run = mm(lower, hi) + mm(lower, lo)
            s_col = spike_col[:, h : h + 1]
            s_row = spike_row[h : h + 1, :]
            q_up = lifted * jnp.exp(run)
            k_down = (intake * jnp.exp(-run)).astype(jnp.bfloat16)
            decay = jnp.exp(jnp.where(causal, s_col - s_row, 0.0))
            inner = jnp.where(causal, mm(q_up.astype(jnp.bfloat16), k_down, NT) * decay, 0.0)
            v = m.pi[part, vs]
            output = mm(inner.astype(jnp.bfloat16), v)
            decayed = q_up * jnp.exp(s_col)
            total = run[part_rows - 1 : part_rows, :] + s_col[part_rows - 1 : part_rows, :]
            k_end = (intake * jnp.exp(total - (run + s_col))).astype(jnp.bfloat16)
            state = mm(v, k_end, TN)
            if which == 0:
                m.local_out[part, vs] = output
                m.qdec[part, ks] = decayed.astype(jnp.bfloat16)
                m.half_state[:, ks] = state
                m.half_total[:, ks] = total
                continue
            earlier = m.half_state[:, ks]
            m.local_out[part, vs] = output + mm(decayed.astype(jnp.bfloat16), earlier.astype(jnp.bfloat16), NT)
            m.qdec[part, ks] = (decayed * jnp.exp(m.half_total[:, ks])).astype(jnp.bfloat16)
            state = (earlier * jnp.exp(total) + state).astype(jnp.bfloat16)
            tail = tail_of(total + m.half_total[:, ks])
            for i in range(GROUP):
                m.s_own[i, 0:span, ks] = state[i * span : (i + 1) * span]
                m.s_own[i, span:, ks] = tail

    first_rows, last_rows = slice(0, part_rows), slice(part_rows, rows)

    for shift in range(1, tp):
        slot = lax.rem(t + tp - shift, tp)
        for r in range(chunks):
            part = slice(r * chunk, (r + 1) * chunk)
            token_copy(shift, r, slot).wait_recv()
            scaled, squares = scale(slot, part)
            m.far_scaled[part] = scaled
            m.square[part] += jnp.broadcast_to(squares, (chunk, LANES))
            if shift == tp - 1:
                inverse = lax.rsqrt(m.square[part, 0:1] * (1.0 / (features * tp)) + epsilon)
                for i, name in enumerate("kv"):
                    whole = getattr(m, "a" + name)[part, :] + mm(
                        m.far_scaled[part], weight_rows(name, slot, slice(0, width))
                    )
                    m.kv[me, part, i * width : (i + 1) * width] = (whole * inverse).astype(jnp.bfloat16)
                relay(z, y, r, lambda one: one.start())
                if 0 < r < chunks - 1:
                    wave_events(1, r - 1)
                if r == chunks // 2 - 1:
                    for name in "qrfi":
                        project(name, first_rows)
                    recur(0)
        if shift < tp - 1:
            for name in order:
                for cut in tiles(name):
                    getattr(m, "a" + name)[:, cut] += mm(m.far_scaled[...], weight_rows(name, slot, cut))
    slot = lax.rem(t + 1, tp)
    def outer_copy(shift, array, other):
        from_columns = array.at[:, pl.ds(pl.multiple_of(partner(shift) * columns, columns), columns)]
        return remote(
            from_columns, m.win.at[t, other], m.outer_send.at[shift - 1, 0], m.outer_recv.at[shift - 1, 0], tp=partner(shift)
        )

    for which, array in enumerate(outer):

        @pl.when(c == which)
        def _():
            start([outer_copy(shift, array, which) for shift in range(1, tp)])

    def outer_share(shift):
        piece = m.win.at[lax.rem(t + tp - shift, tp), c]
        return remote(piece, piece, m.outer_send.at[shift - 1, 1], m.outer_recv.at[shift - 1, 1], sp=sibling)

    def query_copy():
        return remote(m.pq, m.far_q, m.lend_send.at[0], m.lend_recv.at[0], sp=bottom)

    def lent_copy():
        return remote(m.lent, m.lent_back, m.lend_send.at[1], m.lend_recv.at[1], sp=top)

    project("q", last_rows)

    @pl.when(borrows)
    def _():
        query_copy().start()

    for name in "rfi":
        project(name, last_rows)
    wave_events(1, chunks - 2)
    wave_events(2, 0)
    recur(1)

    def s_copy(off):
        return remote(
            m.s_own.at[lax.rem(g + off, GROUP)], m.s_mates.at[g], m.s_send, m.s_recv.at[off - 1], sp=mate(off)
        )

    def p_copy(plane):
        return remote(m.p_own, m.p_planes.at[z], m.p_send.at[plane], m.p_recv.at[z], sp=plane * GROUP + g)

    def p_arrival(plane):
        return remote(m.p_own, m.p_planes.at[plane], m.p_send.at[plane], m.p_recv.at[plane], sp=bottom)

    def i_copy(off):
        return remote(
            m.i_own.at[lax.rem(g + off, GROUP)], m.i_mates.at[g], m.i_send, m.i_recv.at[off - 1], sp=mate(off)
        )

    start([s_copy(off) for off in range(1, GROUP)])
    project("g", slice(0, rows))
    wave_events(1, chunks - 1)
    wave_events(2, 1)
    m.s_mates[g] = m.s_own[g]

    def take_queries(queries):
        for h in range(heads):
            m.qh[h] = queries[:, h * HEAD : (h + 1) * HEAD]

    take_queries(m.pq)

    def parts(packed):
        return packed[0:span].astype(jnp.float32), jnp.sum(packed[span:].astype(jnp.float32), axis=0, keepdims=True)

    def append(state, packed):
        added, total = parts(packed)
        return state * jnp.exp(total) + added

    r_iota, c_iota = iota((rows, rows), 0), iota((rows, rows), 1)
    sums = jnp.where(r_iota > c_iota, -1.0, 0.0).astype(jnp.bfloat16)
    before = c_iota < r_iota

    def attend(numbers, place, first=False, after=False, some=range(heads)):
        scores, stays = [], []
        for number in numbers:
            for h in some:
                hs = slice(h * HEAD, (h + 1) * HEAD)
                s = mm(m.qh[h], m.kv[number, :, hs], NT) * (HEAD**-0.5 * LOG2E) + m.bias[h] * LOG2E
                soft = jnp.maximum(s, jnp.log2(1.0 + jnp.exp2(jnp.minimum(s, 100.0))))
                scores.append(s - soft)
                stays.append(jnp.where(before, soft, 0.0) if first else soft)
        done = {}
        for i, (score, stay) in enumerate(zip(scores, stays)):
            number, h = numbers[i // len(some)], some[i % len(some)]
            vs = slice(width + h * HEAD, width + (h + 1) * HEAD)
            later = mm(stay.astype(jnp.bfloat16), sums)
            w = jnp.exp2(score + later)
            if first:
                w = jnp.where(before, w, 0.0)
            o = mm(w.astype(jnp.bfloat16), m.kv[number, :, vs])
            every = jnp.broadcast_to((later - stay)[:, 0:1], (rows, HEAD))
            if after:
                done[h] = m.part[place, h], m.carry[place, h]
            if h in done:
                o, every = done[h][0] + o * jnp.exp2(done[h][1]), done[h][1] + every
            done[h] = o, every
            if number is numbers[-1]:
                m.part[place, h], m.carry[place, h] = done[h]

    attend([me], 1 - y, first=True)

    @pl.when(c == 1)
    def _():
        from_sibling(z, y)
        attend([me - 1], 1 - y, after=True)

    def combine(place, some=range(heads)):
        for h in some:
            m.part[1 - y, h] += m.part[place, h] * jnp.exp2(m.carry[1 - y, h])
            m.carry[1 - y, h] += m.carry[place, h]

    def combine_wave(w):
        for place in (2 * w - 2, 2 * w - 1):

            @pl.when(place > 1 - y)
            def _():
                combine(place)

    def gather_states():
        for off in range(1, GROUP):
            s_copy(off).wait_recv()
        state, total = parts(m.s_mates[0])
        for i in range(1, GROUP):
            state = append(state, m.s_mates[i])
            total = total + parts(m.s_mates[i])[1]
        m.p_own[0:span] = state.astype(jnp.bfloat16)
        m.p_own[span:] = tail_of(total)

        @pl.loop(z + 1, planes)
        def _(plane):
            p_copy(plane).start()

    def enter_states():
        @pl.loop(0, z)
        def _(plane):
            p_arrival(plane).wait_recv()

        state = lax.fori_loop(
            0, z, lambda plane, so_far: append(so_far, m.p_planes[plane]), jnp.zeros((span, wide), jnp.float32)
        )
        for i in range(GROUP):
            m.i_own[i] = state.astype(jnp.bfloat16)
            state = append(state, m.s_mates[i])
        start([i_copy(off) for off in range(1, GROUP)])
        m.i_mates[g] = m.i_own[g]

    def head_copy(i, shift):
        piece = m.rec.at[t] if i == len(batches) else m.att.at[t, i]
        return remote(piece, piece, m.head_send.at[i, shift - 1], m.head_recv.at[i, shift - 1], tp=partner(shift))

    def finish_states():
        for off in range(1, GROUP):
            i_copy(off).wait_recv()
        for h in range(rec_heads):
            ks = slice(h * REC_KEY, (h + 1) * REC_KEY)
            vs = slice(h * REC_VAL, (h + 1) * REC_VAL)
            entering = jnp.concatenate([m.i_mates[i, :, ks] for i in range(GROUP)], axis=0)
            raw = m.local_out[:, vs] + mm(m.qdec[:, ks], entering, NT)
            gate = m.pg[:, vs].astype(jnp.float32)
            mean = jnp.sum(raw * raw, axis=1, keepdims=True) * (1.0 / REC_VAL)
            done = raw * lax.rsqrt(mean + epsilon) * m.small[1:2, 0:REC_VAL] * (gate * jax.nn.sigmoid(gate))
            m.rec[t, :, vs] = done.astype(jnp.bfloat16)
        start([head_copy(len(batches), shift) for shift in range(1, tp)])

    waves = z + 1 - borrows.astype(jnp.int32)

    @pl.loop(1, waves + 1)
    def _(w):
        @pl.when(w > 1)
        def _():
            combine_wave(w - 1)
            wave_events(w, chunks - 1)

        @pl.when(w == 3)
        def _():
            finish_states()

        @pl.loop(0, 2)
        def _(i):
            zs, ys = z - w + 1 - i, jnp.where(i == 0, 1 - y, y)

            @pl.when((i == 1) & (zs >= 0) & ~(borrows & (zs == 0)) | (i == 0) & ((w > 1) | (y == 1)) & (w < waves))
            def _():
                from_sibling(zs, ys)
                attend([zs * GROUP + ys * 2 + 1, zs * GROUP + ys * 2], 2 * (z - zs) + 1 - ys)

            @pl.when((w == 1) & (i == 0))
            def _():
                for r in range(2, chunks - 1):
                    wave_events(2, r)

            @pl.when((w > 1) & (i == 0))
            def _():
                for r in range(chunks - 1):
                    wave_events(w + 1, r)

            @pl.when((w == 2) & (i == 0))
            def _():
                enter_states()

        @pl.when(w == 1)
        def _():
            gather_states()

    @pl.when(z == 0)
    def _():
        enter_states()

    if lend:

        @pl.when(z == 0)
        def _():
            query_copy().wait_recv()
            take_queries(m.far_q)

            @pl.when(c == 0)
            def _():
                from_sibling(0, y)

            from_sibling(0, 1 - y)

            @pl.loop(0, 2)
            def _(i):
                attend([3 - 2 * i, 2 - 2 * i], 2 + i)

            for h in range(heads):
                whole = m.part[2, h] + m.part[3, h] * jnp.exp2(m.carry[2, h])
                m.lent[:, h * HEAD : (h + 1) * HEAD] = whole.astype(jnp.bfloat16)
            lent_copy().start()
            take_queries(m.pq)

    @pl.when(z < 2)
    def _():
        finish_states()

    for shift in range(1, tp):
        outer_copy(shift, outer[0], 0).wait_recv()
        outer_share(shift).start()
    for one in load_outer:
        one.wait()

    end, last = waves - 1, z - waves + 1
    facing_end = (waves > 1) | (y == 1)

    @pl.when(facing_end & ~lends)
    def _():
        from_sibling(last, 1 - y)

    @pl.when(borrows)
    def _():
        lent_copy().wait_recv()

    for j, some in enumerate(batches):

        @pl.when(facing_end)
        def _():
            attend([last * GROUP + (1 - y) * 2 + 1, last * GROUP + (1 - y) * 2], 2 * end + y, some=some)

        for place in (2 * end, 2 * end + 1):

            @pl.when(place > 1 - y)
            def _():
                combine(place, some)

        @pl.when(borrows)
        def _():
            for h in some:
                lent = m.lent_back[:, h * HEAD : (h + 1) * HEAD].astype(jnp.float32)
                m.part[1 - y, h] += lent * jnp.exp2(m.carry[1 - y, h])

        m.att[t, j] = jnp.concatenate([m.part[1 - y, h] for h in some], axis=1).astype(jnp.bfloat16)
        start([head_copy(j, shift) for shift in range(1, tp)])

    def attention_rows(slot, j):
        return m.win[slot, 0, HEAD * batches[j][0] : HEAD * (batches[j][-1] + 1), :]

    mixed = mm(m.rec[t], m.win[t, 1])
    for j in range(len(batches)):
        mixed = mixed + mm(m.att[t, j], attention_rows(t, j))
    for shift in range(1, tp):
        slot = lax.rem(t + tp - shift, tp)
        outer_share(shift).wait_recv()
        head_copy(len(batches), shift).wait_recv()
        mixed = mixed + mm(m.rec[slot], m.win[slot, 1])
    m.sum[...] = mixed
    for shift in range(1, tp):
        slot = lax.rem(t + tp - shift, tp)
        for j in range(len(batches)):
            head_copy(j, shift).wait_recv()
            mixed = mm(m.att[slot, j], attention_rows(slot, j))
            if shift == tp - 1 and j == len(batches) - 1:
                m.out[...] = (m.sum[...] + mixed).astype(jnp.bfloat16)
            else:
                m.sum[...] += mixed

    for shift in range(1, tp):
        remote(m.tok.at[t], m.tok.at[t], m.tok_send.at[shift - 1], m.tok_recv.at[0, 0], tp=partner(shift)).wait_send()
    several = pl.ds(0, GROUP - 1)
    remote(m.s_own.at[several], m.s_own.at[several], m.s_send, m.s_recv.at[0], sp=sibling).wait_send()
    remote(m.i_own.at[several], m.i_own.at[several], m.i_send, m.i_recv.at[0], sp=sibling).wait_send()
    sent([head_copy(i, shift) for i in range(len(batches) + 1) for shift in range(1, tp)])
    sent([outer_share(shift) for shift in range(1, tp)] + [outer_copy(shift, outer[0], 0) for shift in range(1, tp)])

    @pl.loop(z + 1, planes)
    def _(plane):
        p_copy(plane).wait_send()

    @pl.loop(borrows.astype(jnp.int32), z + 1)
    def _(zs):
        relay(zs, y, None, lambda one: one.wait_send())

        @pl.when((zs < z) | (y == 1) | lends)
        def _():
            relay(zs, 1 - y, None, lambda one: one.wait_send())

    @pl.when(borrows)
    def _():
        query_copy().wait_send()

    @pl.when(lends)
    def _():
        lent_copy().wait_send()


def shards(sp, tp, *arrays):
    (tokens, gain, wq, wk, wv, bias, wr, wf, wi, wg, low, spike, norm, attention_out, recurrence_out) = arrays
    rows, features = tokens.shape
    width, wide, narrow = wq.shape[1], wr.shape[1], wi.shape[1]
    heads = width // HEAD
    columns = attention_out.shape[1] // tp
    chunks = CHUNKS
    planes = sp // GROUP
    batch = min(LANES, width)
    bf16, f32, dma = jnp.bfloat16, jnp.float32, pltpu.SemaphoreType.DMA
    wide_row = gain.shape[0]

    def padded(array, to_rows):
        return jnp.pad(array, ((0, to_rows - array.shape[0]), (0, wide_row - array.shape[1])))

    small = jnp.concatenate(
        [padded(gain[None], 1), padded(norm[None], 7), padded(spike.T, 8), padded(low, 8)], axis=0
    )
    inputs = dict(
        tokens=tokens,
        small=small,
        hbm_k=wk,
        hbm_v=wv,
        hbm_q=wq,
        hbm_r=wr,
        hbm_f=wf,
        hbm_i=wi,
        hbm_g=wg,
        bias=bias,
        hbm_attention_out=attention_out,
        hbm_recurrence_out=recurrence_out,
    )
    in_hbm = [name == "tokens" or name.startswith("hbm") for name in inputs]
    specs = [SMEM if name == "bias" else ANY if hbm else VMEM for name, hbm in zip(inputs, in_hbm)]
    scratch = dict(tok=pltpu.VMEM((tp, rows, features), bf16))
    sizes = dict(k=width, v=width, q=width, r=wide, f=wide, i=narrow, g=narrow)
    for name, size in sizes.items():
        scratch["w" + name] = pltpu.VMEM((features * tp, size), bf16)
        scratch["a" + name] = pltpu.VMEM((rows, size), f32)
        if name in "qrfig":
            scratch["p" + name] = pltpu.VMEM((rows, size), bf16)
    scratch.update(
        own_scaled=pltpu.VMEM((rows, features), bf16),
        far_scaled=pltpu.VMEM((rows, features), bf16),
        square=pltpu.VMEM((rows, LANES), f32),
        kv=pltpu.VMEM((sp, rows, 2 * width), bf16),
        qh=pltpu.VMEM((heads, rows, HEAD), bf16),
        part=pltpu.VMEM((max(4, 2 * planes), heads, rows, HEAD), f32),
        carry=pltpu.VMEM((max(4, 2 * planes), heads, rows, HEAD), f32),
        local_out=pltpu.VMEM((rows, narrow), f32),
        half_state=pltpu.VMEM((REC_VAL, wide), f32),
        half_total=pltpu.VMEM((1, wide), f32),
        qdec=pltpu.VMEM((rows, wide), bf16),
        s_own=pltpu.VMEM((GROUP, REC_VAL // GROUP + TAIL, wide), bf16),
        s_mates=pltpu.VMEM((GROUP, REC_VAL // GROUP + TAIL, wide), bf16),
        p_own=pltpu.VMEM((REC_VAL // GROUP + TAIL, wide), bf16),
        p_planes=pltpu.VMEM((planes, REC_VAL // GROUP + TAIL, wide), bf16),
        i_own=pltpu.VMEM((GROUP, REC_VAL // GROUP, wide), bf16),
        i_mates=pltpu.VMEM((GROUP, REC_VAL // GROUP, wide), bf16),
        win=pltpu.VMEM((tp, 2, width, columns), bf16),
        far_q=pltpu.VMEM((rows, width), bf16),
        lent=pltpu.VMEM((rows, width), bf16),
        lent_back=pltpu.VMEM((rows, width), bf16),
        att=pltpu.VMEM((tp, width // batch, rows, batch), bf16),
        sum=pltpu.VMEM((rows, columns), f32),
        rec=pltpu.VMEM((tp, rows, narrow), bf16),
        load_sem=dma((10,)),
        tok_send=dma((max(tp - 1, 1),)),
        tok_recv=dma((max(tp - 1, 1), chunks)),
        kv_send=dma((3, sp // 2)),
        kv_recv=dma((sp // 2, chunks)),
        sib_recv=dma((sp // 2,)),
        lend_send=dma((2,)),
        lend_recv=dma((2,)),
        s_send=dma,
        s_recv=dma((GROUP - 1,)),
        p_send=dma((planes,)),
        p_recv=dma((planes,)),
        i_send=dma,
        i_recv=dma((GROUP - 1,)),
        outer_send=dma((max(tp - 1, 1), 2)),
        outer_recv=dma((max(tp - 1, 1), 2)),
        head_send=dma((width // batch + 1, max(tp - 1, 1))),
        head_recv=dma((width // batch + 1, max(tp - 1, 1))),
    )
    return pl.pallas_call(
        functools.partial(layer_kernel, sp, tp, list(inputs) + ["out"] + list(scratch)),
        out_shape=jax.ShapeDtypeStruct((rows, columns), bf16),
        in_specs=specs,
        out_specs=VMEM,
        scratch_shapes=list(scratch.values()),
        compiler_params=pltpu.CompilerParams(
            collective_id=0, has_side_effects=True, vmem_limit_bytes=53 * 1024 * 1024
        ),
        name="layer",
    )(*inputs.values())


def solution(mesh):
    placed = (
        P("sp", "tp"),
        P(),
        P(None, "tp"),
        P(None, "tp"),
        P(None, "tp"),
        P("tp"),
        P(None, "tp"),
        P(None, "tp"),
        P(None, "tp"),
        P(None, "tp"),
        P("tp", None),
        P("sp", "tp"),
        P(),
        P("tp", None),
        P("tp", None),
    )
    return jax.shard_map(
        functools.partial(shards, mesh.shape["sp"], mesh.shape["tp"]),
        mesh=mesh,
        in_specs=placed,
        out_specs=P("sp", "tp"),
        check_vma=False,
    )
```

```python
import functools
import math
import types

import jax
import jax.numpy as jnp
from jax import lax
from jax.experimental import pallas as pl
from jax.experimental.pallas import tpu as pltpu
from jax.sharding import PartitionSpec as P

HEAD = 64
REC_KEY = 128
REC_VAL = 64
LANES = 128
GROUP = 4
TAIL = 16
CHUNKS = 4
SPIKES, LOWS = 8, 16
LOG2E = math.log2(math.e)
epsilon = 1e-06
VMEM = pl.BlockSpec(memory_space=pltpu.VMEM)
SMEM = pl.BlockSpec(memory_space=pltpu.SMEM)
ANY = pl.BlockSpec(memory_space=pl.ANY)
NT = (((1,), (1,)), ((), ()))
TN = (((0,), (0,)), ((), ()))


def mm(a, b, dims=(((1,), (0,)), ((), ()))):
    return lax.dot_general(a, b, dims, preferred_element_type=jnp.float32)


def split(x):
    hi = x.astype(jnp.bfloat16)
    return hi, (x - hi.astype(jnp.float32)).astype(jnp.bfloat16)


def iota(shape, dim):
    return lax.broadcasted_iota(jnp.int32, shape, dim)


def start(copies):
    for one in copies:
        one.start()


def sent(copies):
    for one in copies:
        one.wait_send()


def remote(src, dst, send_sem, recv_sem, **target):
    return pltpu.make_async_remote_copy(
        src_ref=src,
        dst_ref=dst,
        send_sem=send_sem,
        recv_sem=recv_sem,
        device_id=target,
        device_id_type=pl.DeviceIdType.MESH,
    )


def tail_of(total):
    hi, lo = split(total)
    lo, rest = split(total - hi.astype(jnp.float32))
    which = iota((TAIL, total.shape[1]), 0)
    tail = jnp.where(which == 0, hi.astype(jnp.float32), jnp.where(which == 1, lo.astype(jnp.float32), 0.0))
    return jnp.where(which == 2, rest.astype(jnp.float32), tail).astype(jnp.bfloat16)


def layer_kernel(sp, tp, names, *refs):
    m = types.SimpleNamespace(**dict(zip(names, refs)))
    rows, features = m.tok.shape[1:]
    width, wide, narrow = m.wk.shape[1], m.wr.shape[1], m.wi.shape[1]
    heads, rec_heads = width // HEAD, narrow // REC_VAL
    chunks, chunk = CHUNKS, rows // CHUNKS
    planes = sp // GROUP
    lend = planes > 2
    columns = m.out.shape[1]
    span = REC_VAL // GROUP
    together = m.att.shape[3] // HEAD
    batches = [range(h, h + together) for h in range(0, heads, together)]
    me, t = lax.axis_index("sp"), lax.axis_index("tp")
    c, y, z = lax.rem(me, 2), lax.rem(me // 2, 2), me // GROUP
    g = lax.rem(me, GROUP)
    sibling, across = me + 1 - 2 * c, z * GROUP + (1 - y) * 2 + c
    ahead = lax.rem(z + 1, planes) * GROUP + g
    bottom, top = g, (planes - 1) * GROUP + g
    lends, borrows = lend & (z == 0), lend & (z == planes - 1)

    def mate(off):
        return z * GROUP + lax.rem(g + off, GROUP)

    def partner(shift):
        return lax.rem(t + shift, tp)

    load_tokens = pltpu.make_async_copy(m.tokens, m.tok.at[t], m.load_sem.at[0])
    load_tokens.start()
    order = "krfivqg"
    loads = [
        pltpu.make_async_copy(getattr(m, "hbm_" + name), getattr(m, "w" + name), m.load_sem.at[1 + i])
        for i, name in enumerate(order)
    ]
    start(loads)
    own_columns = pl.ds(pl.multiple_of(t * columns, columns), columns)
    outer = (m.hbm_attention_out, m.hbm_recurrence_out)
    load_outer = [
        pltpu.make_async_copy(array.at[:, own_columns], m.win.at[t, i], m.load_sem.at[8 + i])
        for i, array in enumerate(outer)
    ]
    start(load_outer)

    barrier = pltpu.get_barrier_semaphore()
    for off in range(1, GROUP):
        pl.semaphore_signal(barrier, inc=1, device_id={"sp": mate(off)}, device_id_type=pl.DeviceIdType.MESH)
    for off in range(1, planes):
        peer = lax.rem(z + off, planes) * GROUP + g
        pl.semaphore_signal(barrier, inc=1, device_id={"sp": peer}, device_id_type=pl.DeviceIdType.MESH)
    for shift in range(1, tp):
        pl.semaphore_signal(barrier, inc=1, device_id={"tp": partner(shift)}, device_id_type=pl.DeviceIdType.MESH)
    pl.semaphore_wait(barrier, GROUP + planes + tp - 3)
    load_tokens.wait()

    def token_copy(shift, r, slot):
        part = m.tok.at[slot, pl.ds(r * chunk, chunk)]
        return remote(part, part, m.tok_send.at[shift - 1], m.tok_recv.at[shift - 1, r], tp=partner(shift))

    token_sends = [token_copy(shift, r, t) for shift in range(1, tp) for r in range(chunks)]
    start(token_sends)

    def scale(slot, part):
        value = m.tok[slot, part, :].astype(jnp.float32)
        gains = m.small[0:1, pl.ds(pl.multiple_of(slot * features, features), features)]
        return (value * gains).astype(jnp.bfloat16), jnp.sum(value * value, axis=1, keepdims=True)

    def weight_rows(name, slot, cut):
        return getattr(m, "w" + name)[pl.ds(pl.multiple_of(slot * features, features), features), cut]

    def tiles(name):
        size = getattr(m, "w" + name).shape[1]
        step = min(256, size)
        return [slice(i, i + step) for i in range(0, size, step)]

    scaled, squares = scale(t, slice(0, rows))
    m.own_scaled[...] = scaled
    m.square[...] = jnp.broadcast_to(squares, m.square.shape)
    for load, name in zip(loads, order):
        load.wait()
        for cut in tiles(name):
            getattr(m, "a" + name)[:, cut] = mm(m.own_scaled[...], weight_rows(name, t, cut))

    def kv_copy(number, r, way, target):
        piece = m.kv.at[number, pl.ds(r * chunk, chunk)]
        kind = number // 2
        if way == 2:
            return remote(piece, piece, m.kv_send.at[2, kind], m.sib_recv.at[kind], sp=target)
        return remote(piece, piece, m.kv_send.at[way, kind], m.kv_recv.at[kind, r], sp=target)

    def kv_whole(number, way):
        piece, kind = m.kv.at[number], number // 2
        return remote(piece, piece, m.kv_send.at[way, kind], m.sib_recv.at[kind], sp=sibling)

    def relay(zs, ys, r, act):
        copy = kv_copy if r is not None else lambda number, r, way, target: kv_whole(number, way)
        number = zs * GROUP + ys * 2 + c
        column, here = ys == y, zs == z
        last = jnp.where(zs == 0, planes - 1 - lend, planes - 1)

        @pl.when(column & (z < last))
        def _():
            act(copy(number, r, 0, ahead))

        @pl.when(column & (~here | (y == 0) | lends))
        def _():
            act(copy(number, r, 1, across))

        @pl.when(~here | (column & (c == 0)) | (~column & (y == 1)) | lends)
        def _():
            act(copy(number, r, 2, sibling))

    def event(cond, zs, ys, r):
        @pl.when(cond & ~(borrows & (zs == 0)))
        def _():
            kv_copy(zs * GROUP + ys * 2 + c, r, 0, ahead).wait_recv()
            relay(zs, ys, r, lambda one: one.start())

    def facing(w):
        return (w <= z + 1) & ((w > 1) | (y == 1) | lends)

    def wave_events(w, r):
        event(w <= z, z - w, y, r)
        event(facing(w), z - w + 1, 1 - y, r)

    def from_sibling(zs, ys):
        kv_whole(zs * GROUP + ys * 2 + 1 - c, 2).wait_recv()

    part_rows = rows // 2
    r_iota, c_iota = iota((part_rows, part_rows), 0), iota((part_rows, part_rows), 1)
    causal = r_iota >= c_iota
    lower = causal.astype(jnp.bfloat16)
    upper = (r_iota <= c_iota).astype(jnp.bfloat16)

    def project(name, part):
        inverse = lax.rsqrt(m.square[part, 0:1] * (1.0 / (features * tp)) + epsilon)
        for cut in tiles(name):
            whole = getattr(m, "a" + name)[part, cut] + mm(
                m.far_scaled[part], weight_rows(name, lax.rem(t + 1, tp), cut)
            )
            getattr(m, "p" + name)[part, cut] = (whole * inverse).astype(jnp.bfloat16)

    def recur(which):
        part = slice(which * part_rows, (which + 1) * part_rows)
        spikes = m.small[SPIKES : SPIKES + rec_heads, part]
        if rec_heads == 1:
            spikes = jnp.broadcast_to(spikes, (8, part_rows))
        hi, lo = split(spikes)
        spike_col = mm(lower, hi, NT) + mm(lower, lo, NT)
        spike_row = mm(hi, upper) + mm(lo, upper)
        for h in range(rec_heads):
            ks = slice(h * REC_KEY, (h + 1) * REC_KEY)
            vs = slice(h * REC_VAL, (h + 1) * REC_VAL)
            q = m.pr[part, ks].astype(jnp.float32)
            lifted = q * jax.nn.sigmoid(q)
            intake = (1.0 - m.small[LOWS + h : LOWS + h + 1, 0:REC_KEY]) * jax.nn.sigmoid(-m.pf[part, ks].astype(jnp.float32))
            hi, lo = split(jnp.log1p(-intake))
            run = mm(lower, hi) + mm(lower, lo)
            s_col = spike_col[:, h : h + 1]
            s_row = spike_row[h : h + 1, :]
            q_up = lifted * jnp.exp(run)
            k_down = (intake * jnp.exp(-run)).astype(jnp.bfloat16)
            decay = jnp.exp(jnp.where(causal, s_col - s_row, 0.0))
            inner = jnp.where(causal, mm(q_up.astype(jnp.bfloat16), k_down, NT) * decay, 0.0)
            v = m.pi[part, vs]
            output = mm(inner.astype(jnp.bfloat16), v)
            decayed = q_up * jnp.exp(s_col)
            total = run[part_rows - 1 : part_rows, :] + s_col[part_rows - 1 : part_rows, :]
            k_end = (intake * jnp.exp(total - (run + s_col))).astype(jnp.bfloat16)
            state = mm(v, k_end, TN)
            if which == 0:
                m.local_out[part, vs] = output
                m.qdec[part, ks] = decayed.astype(jnp.bfloat16)
                m.half_state[:, ks] = state
                m.half_total[:, ks] = total
                continue
            earlier = m.half_state[:, ks]
            m.local_out[part, vs] = output + mm(decayed.astype(jnp.bfloat16), earlier.astype(jnp.bfloat16), NT)
            m.qdec[part, ks] = (decayed * jnp.exp(m.half_total[:, ks])).astype(jnp.bfloat16)
            state = (earlier * jnp.exp(total) + state).astype(jnp.bfloat16)
            tail = tail_of(total + m.half_total[:, ks])
            for i in range(GROUP):
                m.s_own[i, 0:span, ks] = state[i * span : (i + 1) * span]
                m.s_own[i, span:, ks] = tail

    first_rows, last_rows = slice(0, part_rows), slice(part_rows, rows)

    for shift in range(1, tp):
        slot = lax.rem(t + tp - shift, tp)
        for r in range(chunks):
            part = slice(r * chunk, (r + 1) * chunk)
            token_copy(shift, r, slot).wait_recv()
            scaled, squares = scale(slot, part)
            m.far_scaled[part] = scaled
            m.square[part] += jnp.broadcast_to(squares, (chunk, LANES))
            if shift == tp - 1:
                inverse = lax.rsqrt(m.square[part, 0:1] * (1.0 / (features * tp)) + epsilon)
                for i, name in enumerate("kv"):
                    whole = getattr(m, "a" + name)[part, :] + mm(
                        m.far_scaled[part], weight_rows(name, slot, slice(0, width))
                    )
                    m.kv[me, part, i * width : (i + 1) * width] = (whole * inverse).astype(jnp.bfloat16)
                relay(z, y, r, lambda one: one.start())
                if 0 < r < chunks - 1:
                    wave_events(1, r - 1)
                if r == chunks // 2 - 1:
                    for name in "qrfi":
                        project(name, first_rows)
                    recur(0)
        if shift < tp - 1:
            for name in order:
                for cut in tiles(name):
                    getattr(m, "a" + name)[:, cut] += mm(m.far_scaled[...], weight_rows(name, slot, cut))
    slot = lax.rem(t + 1, tp)
    def outer_copy(shift, array, other):
        from_columns = array.at[:, pl.ds(pl.multiple_of(partner(shift) * columns, columns), columns)]
        return remote(
            from_columns, m.win.at[t, other], m.outer_send.at[shift - 1, 0], m.outer_recv.at[shift - 1, 0], tp=partner(shift)
        )

    for which, array in enumerate(outer):

        @pl.when(c == which)
        def _():
            start([outer_copy(shift, array, which) for shift in range(1, tp)])

    def outer_share(shift):
        piece = m.win.at[lax.rem(t + tp - shift, tp), c]
        return remote(piece, piece, m.outer_send.at[shift - 1, 1], m.outer_recv.at[shift - 1, 1], sp=sibling)

    def query_copy():
        return remote(m.pq, m.far_q, m.lend_send.at[0], m.lend_recv.at[0], sp=bottom)

    def lent_copy():
        return remote(m.lent, m.lent_back, m.lend_send.at[1], m.lend_recv.at[1], sp=top)

    project("q", last_rows)

    @pl.when(borrows)
    def _():
        query_copy().start()

    for name in "rfi":
        project(name, last_rows)
    wave_events(2, 0)
    wave_events(1, chunks - 2)
    recur(1)

    def s_copy(off):
        return remote(
            m.s_own.at[lax.rem(g + off, GROUP)], m.s_mates.at[g], m.s_send, m.s_recv.at[off - 1], sp=mate(off)
        )

    def p_copy(plane):
        return remote(m.p_own, m.p_planes.at[z], m.p_send.at[plane], m.p_recv.at[z], sp=plane * GROUP + g)

    def p_arrival(plane):
        return remote(m.p_own, m.p_planes.at[plane], m.p_send.at[plane], m.p_recv.at[plane], sp=bottom)

    def i_copy(off):
        return remote(
            m.i_own.at[lax.rem(g + off, GROUP)], m.i_mates.at[g], m.i_send, m.i_recv.at[off - 1], sp=mate(off)
        )

    start([s_copy(off) for off in range(1, GROUP)])
    project("g", slice(0, rows))
    wave_events(1, chunks - 1)
    wave_events(2, 1)
    m.s_mates[g] = m.s_own[g]

    def take_queries(queries):
        for h in range(heads):
            m.qh[h] = queries[:, h * HEAD : (h + 1) * HEAD]

    take_queries(m.pq)

    def parts(packed):
        return packed[0:span].astype(jnp.float32), jnp.sum(packed[span:].astype(jnp.float32), axis=0, keepdims=True)

    def append(state, packed):
        added, total = parts(packed)
        return state * jnp.exp(total) + added

    r_iota, c_iota = iota((rows, rows), 0), iota((rows, rows), 1)
    sums = jnp.where(r_iota > c_iota, -1.0, 0.0).astype(jnp.bfloat16)
    before = c_iota < r_iota

    def attend(numbers, place, first=False, after=False, some=range(heads)):
        scores, stays = [], []
        for number in numbers:
            for h in some:
                hs = slice(h * HEAD, (h + 1) * HEAD)
                s = mm(m.qh[h], m.kv[number, :, hs], NT) * (HEAD**-0.5 * LOG2E) + m.bias[h] * LOG2E
                soft = jnp.maximum(s, jnp.log2(1.0 + jnp.exp2(jnp.minimum(s, 100.0))))
                scores.append(s - soft)
                stays.append(jnp.where(before, soft, 0.0) if first else soft)
        done = {}
        for i, (score, stay) in enumerate(zip(scores, stays)):
            number, h = numbers[i // len(some)], some[i % len(some)]
            vs = slice(width + h * HEAD, width + (h + 1) * HEAD)
            later = mm(stay.astype(jnp.bfloat16), sums)
            w = jnp.exp2(score + later)
            if first:
                w = jnp.where(before, w, 0.0)
            o = mm(w.astype(jnp.bfloat16), m.kv[number, :, vs])
            every = jnp.broadcast_to((later - stay)[:, 0:1], (rows, HEAD))
            if after:
                done[h] = m.part[place, h], m.carry[place, h]
            if h in done:
                o, every = done[h][0] + o * jnp.exp2(done[h][1]), done[h][1] + every
            done[h] = o, every
            if number is numbers[-1]:
                m.part[place, h], m.carry[place, h] = done[h]

    attend([me], 1 - y, first=True)

    @pl.when(c == 1)
    def _():
        from_sibling(z, y)
        attend([me - 1], 1 - y, after=True)

    def combine(place, some=range(heads)):
        for h in some:
            m.part[1 - y, h] += m.part[place, h] * jnp.exp2(m.carry[1 - y, h])
            m.carry[1 - y, h] += m.carry[place, h]

    def combine_wave(w):
        for place in (2 * w - 2, 2 * w - 1):

            @pl.when(place > 1 - y)
            def _():
                combine(place)

    def gather_states():
        for off in range(1, GROUP):
            s_copy(off).wait_recv()
        state, total = parts(m.s_mates[0])
        for i in range(1, GROUP):
            state = append(state, m.s_mates[i])
            total = total + parts(m.s_mates[i])[1]
        m.p_own[0:span] = state.astype(jnp.bfloat16)
        m.p_own[span:] = tail_of(total)

        @pl.loop(z + 1, planes)
        def _(plane):
            p_copy(plane).start()

    def enter_states():
        @pl.loop(0, z)
        def _(plane):
            p_arrival(plane).wait_recv()

        state = lax.fori_loop(
            0, z, lambda plane, so_far: append(so_far, m.p_planes[plane]), jnp.zeros((span, wide), jnp.float32)
        )
        for i in range(GROUP):
            m.i_own[i] = state.astype(jnp.bfloat16)
            state = append(state, m.s_mates[i])
        start([i_copy(off) for off in range(1, GROUP)])
        m.i_mates[g] = m.i_own[g]

    def head_copy(i, shift):
        piece = m.rec.at[t] if i == len(batches) else m.att.at[t, i]
        return remote(piece, piece, m.head_send.at[i, shift - 1], m.head_recv.at[i, shift - 1], tp=partner(shift))

    def finish_states():
        for off in range(1, GROUP):
            i_copy(off).wait_recv()
        for h in range(rec_heads):
            ks = slice(h * REC_KEY, (h + 1) * REC_KEY)
            vs = slice(h * REC_VAL, (h + 1) * REC_VAL)
            entering = jnp.concatenate([m.i_mates[i, :, ks] for i in range(GROUP)], axis=0)
            raw = m.local_out[:, vs] + mm(m.qdec[:, ks], entering, NT)
            gate = m.pg[:, vs].astype(jnp.float32)
            mean = jnp.sum(raw * raw, axis=1, keepdims=True) * (1.0 / REC_VAL)
            done = raw * lax.rsqrt(mean + epsilon) * m.small[1:2, 0:REC_VAL] * (gate * jax.nn.sigmoid(gate))
            m.rec[t, :, vs] = done.astype(jnp.bfloat16)
        start([head_copy(len(batches), shift) for shift in range(1, tp)])

    waves = z + 1 - borrows.astype(jnp.int32)

    @pl.loop(1, waves + 1)
    def _(w):
        @pl.when(w > 1)
        def _():
            combine_wave(w - 1)
            wave_events(w, chunks - 1)

        @pl.when(w == 3)
        def _():
            finish_states()

        @pl.loop(0, 2)
        def _(i):
            zs, ys = z - w + 1 - i, jnp.where(i == 0, 1 - y, y)

            @pl.when((i == 1) & (zs >= 0) & ~(borrows & (zs == 0)) | (i == 0) & ((w > 1) | (y == 1)) & (w < waves))
            def _():
                from_sibling(zs, ys)
                attend([zs * GROUP + ys * 2 + 1, zs * GROUP + ys * 2], 2 * (z - zs) + 1 - ys)

            @pl.when((w == 1) & (i == 0))
            def _():
                for r in range(2, chunks - 1):
                    wave_events(2, r)

            @pl.when((w > 1) & (i == 0))
            def _():
                for r in range(chunks - 1):
                    wave_events(w + 1, r)

            @pl.when((w == 2) & (i == 0))
            def _():
                enter_states()

        @pl.when(w == 1)
        def _():
            gather_states()

    @pl.when(z == 0)
    def _():
        enter_states()

    if lend:

        @pl.when(z == 0)
        def _():
            query_copy().wait_recv()
            take_queries(m.far_q)

            @pl.when(c == 0)
            def _():
                from_sibling(0, y)

            from_sibling(0, 1 - y)

            @pl.loop(0, 2)
            def _(i):
                attend([3 - 2 * i, 2 - 2 * i], 2 + i)

            for h in range(heads):
                whole = m.part[2, h] + m.part[3, h] * jnp.exp2(m.carry[2, h])
                m.lent[:, h * HEAD : (h + 1) * HEAD] = whole.astype(jnp.bfloat16)
            lent_copy().start()
            take_queries(m.pq)

    @pl.when(z < 2)
    def _():
        finish_states()

    for shift in range(1, tp):
        outer_copy(shift, outer[0], 0).wait_recv()
        outer_share(shift).start()
    for one in load_outer:
        one.wait()

    end, last = waves - 1, z - waves + 1
    facing_end = (waves > 1) | (y == 1)

    @pl.when(facing_end & ~lends)
    def _():
        from_sibling(last, 1 - y)

    @pl.when(borrows)
    def _():
        lent_copy().wait_recv()

    for j, some in enumerate(batches):

        @pl.when(facing_end)
        def _():
            attend([last * GROUP + (1 - y) * 2 + 1, last * GROUP + (1 - y) * 2], 2 * end + y, some=some)

        for place in (2 * end, 2 * end + 1):

            @pl.when(place > 1 - y)
            def _():
                combine(place, some)

        @pl.when(borrows)
        def _():
            for h in some:
                lent = m.lent_back[:, h * HEAD : (h + 1) * HEAD].astype(jnp.float32)
                m.part[1 - y, h] += lent * jnp.exp2(m.carry[1 - y, h])

        m.att[t, j] = jnp.concatenate([m.part[1 - y, h] for h in some], axis=1).astype(jnp.bfloat16)
        start([head_copy(j, shift) for shift in range(1, tp)])

    def attention_rows(slot, j):
        return m.win[slot, 0, HEAD * batches[j][0] : HEAD * (batches[j][-1] + 1), :]

    mixed = mm(m.rec[t], m.win[t, 1])
    for j in range(len(batches)):
        mixed = mixed + mm(m.att[t, j], attention_rows(t, j))
    for shift in range(1, tp):
        slot = lax.rem(t + tp - shift, tp)
        outer_share(shift).wait_recv()
        head_copy(len(batches), shift).wait_recv()
        mixed = mixed + mm(m.rec[slot], m.win[slot, 1])
    m.sum[...] = mixed
    for shift in range(1, tp):
        slot = lax.rem(t + tp - shift, tp)
        for j in range(len(batches)):
            head_copy(j, shift).wait_recv()
            mixed = mm(m.att[slot, j], attention_rows(slot, j))
            if shift == tp - 1 and j == len(batches) - 1:
                m.out[...] = (m.sum[...] + mixed).astype(jnp.bfloat16)
            else:
                m.sum[...] += mixed

    for shift in range(1, tp):
        remote(m.tok.at[t], m.tok.at[t], m.tok_send.at[shift - 1], m.tok_recv.at[0, 0], tp=partner(shift)).wait_send()
    several = pl.ds(0, GROUP - 1)
    remote(m.s_own.at[several], m.s_own.at[several], m.s_send, m.s_recv.at[0], sp=sibling).wait_send()
    remote(m.i_own.at[several], m.i_own.at[several], m.i_send, m.i_recv.at[0], sp=sibling).wait_send()
    sent([head_copy(i, shift) for i in range(len(batches) + 1) for shift in range(1, tp)])
    sent([outer_share(shift) for shift in range(1, tp)] + [outer_copy(shift, outer[0], 0) for shift in range(1, tp)])

    @pl.loop(z + 1, planes)
    def _(plane):
        p_copy(plane).wait_send()

    @pl.loop(borrows.astype(jnp.int32), z + 1)
    def _(zs):
        relay(zs, y, None, lambda one: one.wait_send())

        @pl.when((zs < z) | (y == 1) | lends)
        def _():
            relay(zs, 1 - y, None, lambda one: one.wait_send())

    @pl.when(borrows)
    def _():
        query_copy().wait_send()

    @pl.when(lends)
    def _():
        lent_copy().wait_send()


def shards(sp, tp, *arrays):
    (tokens, gain, wq, wk, wv, bias, wr, wf, wi, wg, low, spike, norm, attention_out, recurrence_out) = arrays
    rows, features = tokens.shape
    width, wide, narrow = wq.shape[1], wr.shape[1], wi.shape[1]
    heads = width // HEAD
    columns = attention_out.shape[1] // tp
    chunks = CHUNKS
    planes = sp // GROUP
    batch = min(LANES, width)
    bf16, f32, dma = jnp.bfloat16, jnp.float32, pltpu.SemaphoreType.DMA
    wide_row = gain.shape[0]

    def padded(array, to_rows):
        return jnp.pad(array, ((0, to_rows - array.shape[0]), (0, wide_row - array.shape[1])))

    small = jnp.concatenate(
        [padded(gain[None], 1), padded(norm[None], 7), padded(spike.T, 8), padded(low, 8)], axis=0
    )
    inputs = dict(
        tokens=tokens,
        small=small,
        hbm_k=wk,
        hbm_v=wv,
        hbm_q=wq,
        hbm_r=wr,
        hbm_f=wf,
        hbm_i=wi,
        hbm_g=wg,
        bias=bias,
        hbm_attention_out=attention_out,
        hbm_recurrence_out=recurrence_out,
    )
    in_hbm = [name == "tokens" or name.startswith("hbm") for name in inputs]
    specs = [SMEM if name == "bias" else ANY if hbm else VMEM for name, hbm in zip(inputs, in_hbm)]
    scratch = dict(tok=pltpu.VMEM((tp, rows, features), bf16))
    sizes = dict(k=width, v=width, q=width, r=wide, f=wide, i=narrow, g=narrow)
    for name, size in sizes.items():
        scratch["w" + name] = pltpu.VMEM((features * tp, size), bf16)
        scratch["a" + name] = pltpu.VMEM((rows, size), f32)
        if name in "qrfig":
            scratch["p" + name] = pltpu.VMEM((rows, size), bf16)
    scratch.update(
        own_scaled=pltpu.VMEM((rows, features), bf16),
        far_scaled=pltpu.VMEM((rows, features), bf16),
        square=pltpu.VMEM((rows, LANES), f32),
        kv=pltpu.VMEM((sp, rows, 2 * width), bf16),
        qh=pltpu.VMEM((heads, rows, HEAD), bf16),
        part=pltpu.VMEM((max(4, 2 * planes), heads, rows, HEAD), f32),
        carry=pltpu.VMEM((max(4, 2 * planes), heads, rows, HEAD), f32),
        local_out=pltpu.VMEM((rows, narrow), f32),
        half_state=pltpu.VMEM((REC_VAL, wide), f32),
        half_total=pltpu.VMEM((1, wide), f32),
        qdec=pltpu.VMEM((rows, wide), bf16),
        s_own=pltpu.VMEM((GROUP, REC_VAL // GROUP + TAIL, wide), bf16),
        s_mates=pltpu.VMEM((GROUP, REC_VAL // GROUP + TAIL, wide), bf16),
        p_own=pltpu.VMEM((REC_VAL // GROUP + TAIL, wide), bf16),
        p_planes=pltpu.VMEM((planes, REC_VAL // GROUP + TAIL, wide), bf16),
        i_own=pltpu.VMEM((GROUP, REC_VAL // GROUP, wide), bf16),
        i_mates=pltpu.VMEM((GROUP, REC_VAL // GROUP, wide), bf16),
        win=pltpu.VMEM((tp, 2, width, columns), bf16),
        far_q=pltpu.VMEM((rows, width), bf16),
        lent=pltpu.VMEM((rows, width), bf16),
        lent_back=pltpu.VMEM((rows, width), bf16),
        att=pltpu.VMEM((tp, width // batch, rows, batch), bf16),
        sum=pltpu.VMEM((rows, columns), f32),
        rec=pltpu.VMEM((tp, rows, narrow), bf16),
        load_sem=dma((10,)),
        tok_send=dma((max(tp - 1, 1),)),
        tok_recv=dma((max(tp - 1, 1), chunks)),
        kv_send=dma((3, sp // 2)),
        kv_recv=dma((sp // 2, chunks)),
        sib_recv=dma((sp // 2,)),
        lend_send=dma((2,)),
        lend_recv=dma((2,)),
        s_send=dma,
        s_recv=dma((GROUP - 1,)),
        p_send=dma((planes,)),
        p_recv=dma((planes,)),
        i_send=dma,
        i_recv=dma((GROUP - 1,)),
        outer_send=dma((max(tp - 1, 1), 2)),
        outer_recv=dma((max(tp - 1, 1), 2)),
        head_send=dma((width // batch + 1, max(tp - 1, 1))),
        head_recv=dma((width // batch + 1, max(tp - 1, 1))),
    )
    return pl.pallas_call(
        functools.partial(layer_kernel, sp, tp, list(inputs) + ["out"] + list(scratch)),
        out_shape=jax.ShapeDtypeStruct((rows, columns), bf16),
        in_specs=specs,
        out_specs=VMEM,
        scratch_shapes=list(scratch.values()),
        compiler_params=pltpu.CompilerParams(
            collective_id=0, has_side_effects=True, vmem_limit_bytes=53 * 1024 * 1024
        ),
        name="layer",
    )(*inputs.values())


def solution(mesh):
    placed = (
        P("sp", "tp"),
        P(),
        P(None, "tp"),
        P(None, "tp"),
        P(None, "tp"),
        P("tp"),
        P(None, "tp"),
        P(None, "tp"),
        P(None, "tp"),
        P(None, "tp"),
        P("tp", None),
        P("sp", "tp"),
        P(),
        P("tp", None),
        P("tp", None),
    )
    return jax.shard_map(
        functools.partial(shards, mesh.shape["sp"], mesh.shape["tp"]),
        mesh=mesh,
        in_specs=placed,
        out_specs=P("sp", "tp"),
        check_vma=False,
    )
```
